256 devices in a mesh: sp: 32 (over z, x), tp: 8 (over y, core).
Axes of the slice: x: 4, y: 4, z: 8, core: 2. Of those that a mesh axis runs over, the one named last changes fastest.
Arguments:
- sequence_embeddings: bfloat16 [12288, 2048], P('sp'), may hold values from -6 to 6
- entry_rescale_vector: bfloat16 [2048], replicated, may hold values from 0.099609375 to 1.8984375
- probe_matrix: bfloat16 [2048, 1024], P('sp', 'tp'), may hold values from -0.125 to 0.125
- onward_retain_matrix: bfloat16 [2048, 1024], P('sp', 'tp'), may hold values from -0.125 to 0.125
- reverse_retain_matrix: bfloat16 [2048, 1024], P('sp', 'tp'), may hold values from -0.125 to 0.125
- content_matrix: bfloat16 [2048, 1024], P('sp', 'tp'), may hold values from -0.125 to 0.125
- emission_switch_matrix: bfloat16 [2048, 1024], P('sp', 'tp'), may hold values from -0.125 to 0.125
- pointwise_content_matrix: bfloat16 [2048, 1024], P('sp', 'tp'), may hold values from -0.125 to 0.125
- pointwise_switch_matrix: bfloat16 [2048, 1024], P('sp', 'tp'), may hold values from -0.125 to 0.125
- retain_lower_slack: float32 [2, 1024], P(None, 'tp'), may hold values from 0 to 0.034, as said below
- extra_log_shrink: float32 [2, 12288, 8], P(None, 'sp', 'tp'), may hold values from -1 to 0
- subspace_rescale: bfloat16 [128], replicated, may hold values from 0.099609375 to 1.8984375
- filter_kernel_coefs: bfloat16 [31, 1024], P(None, 'tp'), may hold values from -1 to 1
- channel_cluster_scale: bfloat16 [1024], P('tp'), may hold values from 0.099609375 to 1.8984375
- scan_readout_matrix: bfloat16 [1024, 2048], P('tp', 'sp'), may hold values from -0.125 to 0.125
- filter_readout_matrix: bfloat16 [1024, 2048], P('tp', 'sp'), may hold values from -0.125 to 0.125
Outputs:
- mixed: bfloat16 [12288, 2048], P(('sp', 'tp'))
The draws below stay inside these ranges and needn't reach their ends.
Inputs may be any that keep to these rules, and one draw needn't show every extreme that they name: `retain_lower_slack`: every entry is positive.
All inputs are finite; a program needn't handle non-finite values.
Results may differ from the reference program's by a relative error of at most 0.015.
Values may be sent and summed in bfloat16 or wider, within the bound.
No kernel may reach another device: no remote copies, remote signals or barrier semaphores. Data moves between devices by JAX's collectives and lax.ppermute only.
A program may use at most 64 MiB of HBM per device.

```python
import math
import jax
import jax.numpy as jnp
from jax import lax

SCAN_SUBSPACES = 8
KEY_DIM = 128
VALUE_DIM = 128
GROUP_CH = 128
CONV_KW = 31
BLOCK = 64
TOK_DEV = 384
KEY_WIDTH = 1024
REC_WIDTH = 1024
CONV_CH = 1024
D = 2048
TOKENS = 12288


def draw_retain_lower_slack(key, part):
    slow_count = SCAN_SUBSPACES // 2
    order_key = jax.random.fold_in(key, 11)
    fast_key = jax.random.fold_in(key, 12)
    slow_key = jax.random.fold_in(key, 13)
    head_ranks = jnp.stack([jax.random.permutation(jax.random.fold_in(order_key, 1), SCAN_SUBSPACES), jax.random.permutation(jax.random.fold_in(order_key, 2), SCAN_SUBSPACES)])
    is_slow = (head_ranks < slow_count)[:, :, None]
    fast_rate = jnp.exp(jax.random.uniform(fast_key, (2, SCAN_SUBSPACES, KEY_DIM), jnp.float32, math.log(0.01), math.log(0.033)))
    slow_rate = jnp.exp(jax.random.uniform(slow_key, (2, SCAN_SUBSPACES, KEY_DIM), jnp.float32, math.log(0.1), math.log(0.5))) / TOKENS
    return jnp.where(is_slow, slow_rate, fast_rate).reshape(2, SCAN_SUBSPACES * KEY_DIM).astype(jnp.float32)


def draw_extra_log_shrink(key, part):
    level_key = jax.random.fold_in(key, 21)
    place_key = jax.random.fold_in(key, 22)
    depth_key = jax.random.fold_in(key, 23)
    device_levels = jnp.exp(jax.random.uniform(level_key, (2, TOKENS // TOK_DEV, SCAN_SUBSPACES), jnp.float32, math.log(0.1), math.log(0.4))) / TOKENS
    constant_level = -jnp.repeat(device_levels, TOK_DEV, axis=1)
    places = jnp.stack([jnp.stack([jax.random.permutation(jax.random.fold_in(place_key, direction * SCAN_SUBSPACES + head), TOKENS)[:3] for head in range(SCAN_SUBSPACES)], axis=1) for direction in range(2)])
    network_levels = jnp.log(jax.random.uniform(depth_key, (2, 3, SCAN_SUBSPACES), jnp.float32, 0.55, 0.8))
    positions = jnp.arange(TOKENS)[None, :, None, None]
    agreement_tally = positions == places[:, None, :, :]
    extra_log_draws = jnp.sum(jnp.where(agreement_tally, network_levels[:, None, :, :], 0.0), axis=2)
    return (constant_level + extra_log_draws).astype(jnp.float32)


def block_scale(rng, shape, shards, smallest, high):
    loudness = 1.0
    for position, parts in shards:
        steps = jax.random.uniform(jax.random.fold_in(jax.random.fold_in(rng, 6), position), (parts,), jnp.float32, smallest / len(shards), high / len(shards))
        loudness = loudness * jnp.repeat(jnp.exp(steps), shape[position] // parts).reshape((-1,) + (1,) * (len(shape) - 1 - position))
    return loudness


def normal_values(rng, dims, width, bound, pieces=(), held_as=jnp.bfloat16):
    array = jax.random.normal(rng, dims, jnp.float32) * width
    if len(pieces) > 0:
        array = block_scale(rng, dims, pieces, -0.22, 0.18) * array
    return jnp.clip(array, min=-bound, max=bound).astype(held_as)


def setup_inputs(seed: int = 0) -> dict:
    streams_of = jax.random.split(jax.random.key(seed), 17)
    return {
        "sequence_embeddings": normal_values(streams_of[0], (TOKENS, D), 1.0, 6.0, ((0, 32),)),
        "entry_rescale_vector": jnp.clip(1.0 + 0.18 * jax.random.normal(streams_of[1], (D,), jnp.float32), 0.099609375, 1.8984375).astype(jnp.bfloat16),
        "probe_matrix": normal_values(streams_of[2], (D, KEY_WIDTH), D ** -0.5, 0.125, ((0, 32), (1, 8))),
        "onward_retain_matrix": normal_values(streams_of[3], (D, KEY_WIDTH), D ** -0.5, 0.125, ((0, 32), (1, 8))),
        "reverse_retain_matrix": normal_values(streams_of[4], (D, KEY_WIDTH), D ** -0.5, 0.125, ((0, 32), (1, 8))),
        "content_matrix": normal_values(streams_of[5], (D, REC_WIDTH), D ** -0.5, 0.125, ((0, 32), (1, 8))),
        "emission_switch_matrix": normal_values(streams_of[6], (D, REC_WIDTH), D ** -0.5, 0.125, ((0, 32), (1, 8))),
        "pointwise_content_matrix": normal_values(streams_of[7], (D, CONV_CH), D ** -0.5, 0.125, ((0, 32), (1, 8))),
        "pointwise_switch_matrix": normal_values(streams_of[8], (D, CONV_CH), D ** -0.5, 0.125, ((0, 32), (1, 8))),
        "retain_lower_slack": draw_retain_lower_slack(jax.random.fold_in(streams_of[16], 71), 0),
        "extra_log_shrink": draw_extra_log_shrink(jax.random.fold_in(streams_of[16], 71), 0),
        "subspace_rescale": jnp.clip(1.0 + 0.18 * jax.random.normal(streams_of[11], (VALUE_DIM,), jnp.float32), 0.099609375, 1.8984375).astype(jnp.bfloat16),
        "filter_kernel_coefs": normal_values(streams_of[12], (CONV_KW, CONV_CH), CONV_KW ** -0.5, 1.0, ((1, 8),)),
        "channel_cluster_scale": jnp.clip(1.0 + 0.18 * jax.random.normal(streams_of[13], (CONV_CH,), jnp.float32), 0.099609375, 1.8984375).astype(jnp.bfloat16),
        "scan_readout_matrix": normal_values(streams_of[14], (REC_WIDTH, D), D ** -0.5, 0.125, ((0, 8), (1, 32))),
        "filter_readout_matrix": normal_values(streams_of[15], (CONV_CH, D), D ** -0.5, 0.125, ((0, 8), (1, 32))),
    }


precise_setting = lax.Precision.HIGHEST

def normalize(sequence_embeddings, entry_rescale_vector):
    floats = sequence_embeddings.astype(jnp.float32)
    factor = lax.rsqrt(lax.optimization_barrier(jnp.mean(floats * floats, axis=-1, keepdims=True)) + 1e-06)
    return (floats * factor * entry_rescale_vector.astype(jnp.float32)).astype(jnp.bfloat16)

def sigmoid_switch_entries(emission_switch_scores, retain_lower_slack_line, drawn_extra_lines, subspace_amount):
    length = emission_switch_scores.shape[0]
    retain_slack_amount = retain_lower_slack_line.astype(jnp.float32)[None, :] * jax.nn.sigmoid(-emission_switch_scores)
    retain_slack_amount = retain_slack_amount.reshape(length, subspace_amount, -1)
    log_shrink_amount = jnp.log1p(-retain_slack_amount) + drawn_extra_lines.astype(jnp.float32)[:, :, None]
    return (log_shrink_amount, retain_slack_amount)

def block_recurrence(queries, log_shrink_amount, retain_slack_amount, value_rows, initial):
    length, subspace_amount, key_dim = queries.shape
    block_count = length // BLOCK

    def to_blocks(tensor):
        return tensor.reshape(block_count, BLOCK, subspace_amount, tensor.shape[-1])
    lower_mask = jnp.tril(jnp.ones((BLOCK, BLOCK), jnp.float32))

    def advance(state_carried_over, blocked):
        query_block, decay_block, gap_block, value_block_rows = blocked
        running_state = jnp.cumsum(decay_block, axis=0)
        block_grand_total = running_state[-1]
        lifted_values = query_block * jnp.exp(running_state)
        lowered = gap_block * jnp.exp(-running_state)
        scores = jnp.einsum('thk,shk->hts', lifted_values, lowered, precision=precise_setting) * lower_mask
        within_block = jnp.einsum('hts,shv->thv', scores, value_block_rows, precision=precise_setting)
        output_rows = within_block + jnp.einsum('ipm,pmo->ipo', lifted_values, state_carried_over, precision=precise_setting)
        fading_factor = gap_block * jnp.exp(block_grand_total - running_state)
        updated_state = jnp.exp(block_grand_total)[:, :, None] * state_carried_over + jnp.einsum('fwd,fwt->wdt', fading_factor, value_block_rows, precision=precise_setting)
        return (updated_state, output_rows)
    last_state, output_rows = lax.scan(advance, initial, (to_blocks(queries), to_blocks(log_shrink_amount), to_blocks(retain_slack_amount), to_blocks(value_rows)))
    return (output_rows.reshape(length, subspace_amount, value_rows.shape[-1]), last_state)

def readout(summed, subspace_rescale, out_gate):
    length = summed.shape[0]
    factor = lax.rsqrt(lax.optimization_barrier(jnp.mean(summed * summed, axis=-1, keepdims=True)) + 1e-06)
    scaled = summed * factor * subspace_rescale.astype(jnp.float32)
    return (scaled.reshape(length, -1) * jax.nn.silu(out_gate)).astype(jnp.bfloat16)

def depthwise(framed, filter_kernel_coefs):
    channels = framed.shape[1]
    result = lax.conv_general_dilated(framed[None], filter_kernel_coefs[:, None, :], (1,), 'VALID', dimension_numbers=('NWC', 'WIO', 'NWC'), feature_group_count=channels, preferred_element_type=jnp.float32)
    return result[0]

def group_norm_silu(conv_sum, channel_cluster_scale):
    length, channels = conv_sum.shape
    grouped = conv_sum.reshape(length, -1, GROUP_CH)
    centred = grouped - lax.optimization_barrier(jnp.mean(grouped, axis=-1, keepdims=True))
    variance = lax.optimization_barrier(jnp.mean(centred * centred, axis=-1, keepdims=True))
    standard = (centred * lax.rsqrt(variance + 1e-05)).reshape(length, channels)
    return jax.nn.silu(standard * channel_cluster_scale.astype(jnp.float32)).astype(jnp.bfloat16)

def reference(sequence_embeddings, entry_rescale_vector, probe_matrix, onward_retain_matrix, reverse_retain_matrix, content_matrix, emission_switch_matrix, pointwise_content_matrix, pointwise_switch_matrix, retain_lower_slack, extra_log_shrink, subspace_rescale, filter_kernel_coefs, channel_cluster_scale, scan_readout_matrix, filter_readout_matrix):
    normed = normalize(sequence_embeddings, entry_rescale_vector)

    def multiply_by_matrix(matrix):
        return jnp.dot(normed, matrix, preferred_element_type=jnp.float32)
    length = sequence_embeddings.shape[0]
    queries = jax.nn.silu(multiply_by_matrix(probe_matrix)).reshape(length, SCAN_SUBSPACES, KEY_DIM)
    value_rows = multiply_by_matrix(content_matrix).reshape(length, SCAN_SUBSPACES, VALUE_DIM)
    onward_shrink_multiplier, onward_retain_slack = sigmoid_switch_entries(multiply_by_matrix(onward_retain_matrix), retain_lower_slack[0], extra_log_shrink[0], SCAN_SUBSPACES)
    reverse_shrink_multiplier, reverse_retain_slack = sigmoid_switch_entries(multiply_by_matrix(reverse_retain_matrix), retain_lower_slack[1], extra_log_shrink[1], SCAN_SUBSPACES)
    zero_state = jnp.zeros((SCAN_SUBSPACES, KEY_DIM, VALUE_DIM), jnp.float32)
    forward_out = block_recurrence(queries, onward_shrink_multiplier, onward_retain_slack, value_rows, zero_state)[0]
    backward_out = block_recurrence(jnp.flip(queries, 0), jnp.flip(reverse_shrink_multiplier, 0), jnp.flip(reverse_retain_slack, 0), jnp.flip(value_rows, 0), zero_state)[0]
    backward_out = jnp.flip(backward_out, 0)
    rec_out = readout(forward_out + backward_out, subspace_rescale, multiply_by_matrix(emission_switch_matrix))
    glu = (multiply_by_matrix(pointwise_content_matrix) * jax.nn.sigmoid(multiply_by_matrix(pointwise_switch_matrix))).astype(jnp.bfloat16)
    reach = CONV_KW // 2
    framed = jnp.pad(glu, ((reach, reach), (0, 0)))
    conv_out = group_norm_silu(depthwise(framed, filter_kernel_coefs), channel_cluster_scale)
    mixed = jnp.dot(rec_out, scan_readout_matrix, preferred_element_type=jnp.float32) + jnp.dot(conv_out, filter_readout_matrix, preferred_element_type=jnp.float32)
    return mixed.astype(jnp.bfloat16)
```

```python
import functools

import jax
import jax.numpy as jnp
from jax import lax
from jax.experimental import pallas as pl
from jax.experimental.pallas import tpu as pltpu
from jax.sharding import Mesh
from jax.sharding import PartitionSpec as P


CONV_KW = 31
BLOCK = 64
HEAD = 128
BF = jnp.bfloat16
F32 = jnp.float32


def ring(count, step):
    return [(i, (i + step) % count) for i in range(count)]


def shift(array, axis, step):
    return lax.ppermute(array, axis, ring(lax.axis_size(axis), step))


def line(array, axes, step):
    count = lax.axis_size(axes)
    pairs = [(i, i + step) for i in range(count) if 0 <= i + step < count]
    return lax.ppermute(array, axes, pairs)


def ring_gather(block, axis):
    up, down = [block], [block]
    for _ in range(3):
        up.append(shift(up[-1], axis, 1))
        down.append(shift(down[-1], axis, -1))
    half = block.shape[0] // 2
    far = jnp.concatenate(
        [shift(up[3][:half], axis, 1), shift(down[3][half:], axis, -1)], axis=0
    )
    return [block, down[1], down[2], down[3], far, up[3], up[2], up[1]]


def normalize_kernel(place, x, gain, out):
    z, turn = place[0], place[1]
    floats = x[...].astype(F32)
    factor = lax.rsqrt(jnp.mean(floats * floats, axis=-1, keepdims=True) + 1e-06)
    for k in range(8):
        at = pl.multiple_of(lax.rem(z + k, 8) * 256, 256)
        piece = x[:, pl.ds(at, 256)].astype(F32)
        scaled = piece * factor * gain[:, pl.ds(at, 256)].astype(F32)
        out[:, k * 256 : (k + 1) * 256] = pltpu.roll(scaled, turn, 1).astype(BF)


def normalized(x, gain):
    place = jnp.stack([lax.axis_index("z"), lax.rem(4 - lax.axis_index("x"), 4) * 64])
    return pl.pallas_call(
        normalize_kernel,
        out_shape=jax.ShapeDtypeStruct(x.shape, BF),
        in_specs=[
            pl.BlockSpec(memory_space=pltpu.SMEM),
            pl.BlockSpec(memory_space=pltpu.VMEM),
            pl.BlockSpec(memory_space=pltpu.VMEM),
        ],
        out_specs=pl.BlockSpec(memory_space=pltpu.VMEM),
        name="normalize",
    )(place.astype(jnp.int32), x, gain[None])


def nt(a, b):
    return lax.dot_general(a, b, (((1,), (1,)), ((), ())), preferred_element_type=F32)


def tn(a, b):
    return lax.dot_general(a, b, (((0,), (0,)), ((), ())), preferred_element_type=F32)


def gates_kernel(scores_f, scores_b, values, slack, extra, gap_o, cum_o, start_o, end_o, decay_o):
    length = values.shape[0]
    blocks = length // BLOCK
    inside = lax.rem(lax.broadcasted_iota(jnp.int32, (length, HEAD), 0), BLOCK)
    v = values[...].astype(BF)
    for d, scores in enumerate((scores_f, scores_b)):
        gap = slack[d : d + 1, :] * jax.nn.sigmoid(-scores[...])
        cum = jnp.log1p(-gap) + extra[d]
        step = 1
        while step < BLOCK:
            if d == 0:
                moved = jnp.where(inside >= step, pltpu.roll(cum, step, 0), 0.0)
            else:
                moved = jnp.where(inside < BLOCK - step, pltpu.roll(cum, length - step, 0), 0.0)
            cum = cum + moved
            step *= 2
        gap_o[d] = gap
        cum_o[d] = cum
        state = jnp.zeros((HEAD, HEAD), F32)
        passed = jnp.zeros((1, HEAD), F32)
        for n in range(blocks) if d == 0 else reversed(range(blocks)):
            rows = slice(n * BLOCK, (n + 1) * BLOCK)
            last = n * BLOCK + (BLOCK - 1 if d == 0 else 0)
            total = cum[last : last + 1]
            fade = gap[rows] * jnp.exp(total - cum[rows])
            start_o[d, n] = state.astype(BF)
            decay_o[d, n : n + 1] = passed
            state = jnp.exp(total) * state + tn(v[rows], fade.astype(BF))
            passed = passed + total
        end_o[d] = state
        decay_o[d, blocks : blocks + 1] = passed
        decay_o[d, blocks + 1 : blocks + 2] = passed


def gates(scores_f, scores_b, values, slack, extra):
    length = values.shape[0]
    blocks = length // BLOCK
    return pl.pallas_call(
        gates_kernel,
        out_shape=(
            jax.ShapeDtypeStruct((2, length, HEAD), F32),
            jax.ShapeDtypeStruct((2, length, HEAD), F32),
            jax.ShapeDtypeStruct((2, blocks, HEAD, HEAD), BF),
            jax.ShapeDtypeStruct((2, HEAD, HEAD), F32),
            jax.ShapeDtypeStruct((2, blocks + 2, HEAD), F32),
        ),
        name="gates",
    )(scores_f, scores_b, values, slack, extra)


def local_kernel(pre_query, values, gap, cum, start, decay, out, lifted_o):
    length = values.shape[0]
    blocks = length // BLOCK
    t = lax.broadcasted_iota(jnp.int32, (BLOCK, BLOCK), 0)
    s = lax.broadcasted_iota(jnp.int32, (BLOCK, BLOCK), 1)
    for n in range(blocks):
        rows = slice(n * BLOCK, (n + 1) * BLOCK)
        pre = pre_query[rows]
        q = pre * jax.nn.sigmoid(pre)
        v = values[rows].astype(BF)
        total = jnp.zeros((BLOCK, HEAD), F32)
        for d in range(2):
            c = cum[d, rows]
            lifted = q * jnp.exp(c)
            lowered = gap[d, rows] * jnp.exp(-c)
            scores = nt(lifted.astype(BF), lowered.astype(BF))
            scores = jnp.where(s <= t if d == 0 else s >= t, scores, 0.0)
            total = total + jnp.dot(scores.astype(BF), v, preferred_element_type=F32)
            total = total + nt(lifted.astype(BF), start[d, n])
            lifted_o[d, rows] = (lifted * jnp.exp(decay[d, n : n + 1])).astype(BF)
        out[rows] = total


def local_rows(pre_query, values, gap, cum, start, decay):
    length = values.shape[0]
    return pl.pallas_call(
        local_kernel,
        out_shape=(
            jax.ShapeDtypeStruct((length, HEAD), F32),
            jax.ShapeDtypeStruct((2, length, HEAD), BF),
        ),
        name="local",
    )(pre_query, values, gap, cum, start, decay)


def readout_kernel(local, lifted, incoming, rescale, out_gate, out):
    summed = local[...] + nt(lifted[0], incoming[0]) + nt(lifted[1], incoming[1])
    factor = lax.rsqrt(jnp.mean(summed * summed, axis=-1, keepdims=True) + 1e-06)
    gate = out_gate[...]
    scaled = summed * factor * rescale[...].astype(F32)
    out[...] = (scaled * (gate * jax.nn.sigmoid(gate))).astype(BF)


def readout(local, lifted, incoming, rescale, out_gate):
    return pl.pallas_call(
        readout_kernel,
        out_shape=jax.ShapeDtypeStruct(local.shape, BF),
        name="readout",
    )(local, lifted, incoming, rescale[None], out_gate)


def split_log(log):
    high = log.astype(BF)
    return high, (log - high.astype(F32)).astype(BF)


def packed(state, log):
    high, low = split_log(log)
    logs = jnp.stack([high, low], axis=-2)
    pad = jnp.zeros((*logs.shape[:-2], 14, logs.shape[-1]), BF)
    return jnp.concatenate([state.astype(BF), logs, pad], axis=-2)


def unpacked(message):
    rows = message.shape[-2] - 16
    log = message[..., rows, :].astype(F32) + message[..., rows + 1, :].astype(F32)
    return message[..., :rows, :].astype(F32), log


def scan_states(states, logs, reverse):
    count = states.shape[0]
    order = list(reversed(range(count))) if reverse else list(range(count))
    before, passed = {}, {}
    state, log = jnp.zeros_like(states[0]), jnp.zeros_like(logs[0])
    for k in order:
        before[k], passed[k] = state, log
        state = jnp.exp(logs[k])[None, :] * state + states[k]
        log = log + logs[k]
    return [before[k] for k in range(count)], [passed[k] for k in range(count)], state, log


def exchange(ends, logs):
    quarters = ends.reshape(2, 4, 32, HEAD).swapaxes(0, 1)
    message = packed(quarters, jnp.broadcast_to(logs[None], (4, 2, HEAD)))
    got = lax.all_to_all(message, "x", 0, 0, tiled=True)
    states, steps = unpacked(got)
    rows = []
    for d in range(2):
        rows.append(scan_states(states[:, d], steps[:, d], d == 1))
    totals = packed(jnp.stack([r[2] for r in rows]), jnp.stack([r[3] for r in rows]))
    every = lax.all_to_all(
        jnp.broadcast_to(totals[None], (8, *totals.shape)), "z", 0, 0, tiled=True
    )
    z_states, z_steps = unpacked(every)
    z = lax.axis_index("z")
    back = []
    for d in range(2):
        state = jnp.zeros_like(z_states[0, d])
        for k in range(8) if d == 0 else reversed(range(8)):
            passed = k < z if d == 0 else k > z
            new = jnp.exp(z_steps[k, d])[None, :] * state + z_states[k, d]
            state = jnp.where(passed, new, state)
        before, passed_logs = rows[d][0], rows[d][1]
        back.append(
            jnp.stack([before[k] + jnp.exp(passed_logs[k])[None, :] * state for k in range(4)])
        )
    home = lax.all_to_all(jnp.stack(back, axis=1).astype(BF), "x", 0, 0, tiled=True)
    return home.swapaxes(0, 1).reshape(2, HEAD, HEAD)


def depthwise(framed, filter_kernel_coefs):
    channels = framed.shape[1]
    result = lax.conv_general_dilated(
        framed[None],
        filter_kernel_coefs[:, None, :],
        (1,),
        "VALID",
        dimension_numbers=("NWC", "WIO", "NWC"),
        feature_group_count=channels,
        preferred_element_type=F32,
    )
    return result[0]


def group_norm_silu(conv_sum, channel_cluster_scale):
    centred = conv_sum - jnp.mean(conv_sum, axis=-1, keepdims=True)
    variance = jnp.mean(centred * centred, axis=-1, keepdims=True)
    standard = centred * lax.rsqrt(variance + 1e-05)
    return jax.nn.silu(standard * channel_cluster_scale.astype(F32)).astype(BF)


def project(rows, blocks):
    total = None
    for k, block in enumerate(blocks):
        part = jnp.dot(
            rows[:, k * 256 : (k + 1) * 256], block, preferred_element_type=F32
        )
        total = part if total is None else total + part
    return total


def on_device(
    sequence_embeddings,
    entry_rescale_vector,
    probe_matrix,
    onward_retain_matrix,
    reverse_retain_matrix,
    content_matrix,
    emission_switch_matrix,
    pointwise_content_matrix,
    pointwise_switch_matrix,
    retain_lower_slack,
    extra_log_shrink,
    subspace_rescale,
    filter_kernel_coefs,
    channel_cluster_scale,
    scan_readout_matrix,
    filter_readout_matrix,
):
    readouts = jnp.concatenate([scan_readout_matrix, filter_readout_matrix], axis=0)
    shard = jnp.concatenate(
        [
            onward_retain_matrix,
            reverse_retain_matrix,
            content_matrix,
            probe_matrix,
            emission_switch_matrix,
            pointwise_content_matrix,
            pointwise_switch_matrix,
            readouts.T,
        ],
        axis=1,
    )
    near = [shard, shift(shard, "x", -1), shift(shard, "x", 2), shift(shard, "x", 1)]
    first = jnp.concatenate([piece[:, :384] for piece in near], axis=0)
    later = jnp.concatenate([piece[:, 384:] for piece in near], axis=0)
    normed = normalized(sequence_embeddings, entry_rescale_vector)
    first_blocks = ring_gather(first, "z")
    later, *first_blocks = lax.optimization_barrier((later, *first_blocks))
    later_blocks = ring_gather(later, "z")

    scores = project(normed, first_blocks)
    values = scores[:, 256:384]
    gap, cum, start, end, decay = gates(
        scores[:, :128], scores[:, 128:256], values, retain_lower_slack, extra_log_shrink
    )
    incoming = exchange(end, decay[:, -1])

    later_scores = project(normed, [block[:, :512] for block in later_blocks])
    pre_query, out_gate, glu_a, glu_b = (later_scores[:, k * 128 : (k + 1) * 128] for k in range(4))
    glu = (glu_a * jax.nn.sigmoid(glu_b)).astype(BF)
    reach = CONV_KW // 2
    low = line(glu[-reach:], ("z", "x"), 1)
    high = line(glu[:reach], ("z", "x"), -1)
    framed = jnp.concatenate([low, glu, high], axis=0)
    conv_out = group_norm_silu(depthwise(framed, filter_kernel_coefs), channel_cluster_scale)
    local, lifted = local_rows(pre_query, values, gap, cum, start, decay)
    rec_out = readout(local, lifted, incoming, subspace_rescale, out_gate)

    columns = jnp.stack([block[:, 512:].reshape(4, 64, 256) for block in later_blocks])
    columns = jnp.roll(columns, (lax.axis_index("z"), lax.axis_index("x")), axis=(0, 1))
    columns = columns.reshape(2048, 256)
    part = nt(rec_out, columns[:, :128]) + nt(conv_out, columns[:, 128:])
    part = part.reshape(4, 2, 48, 2048)
    core = lax.axis_index("core")
    mine = lax.dynamic_index_in_dim(part, core, 1, False)
    theirs = lax.dynamic_index_in_dim(part, 1 - core, 1, False).astype(BF)
    both = mine + shift(theirs, "core", 1).astype(F32)
    pieces = lax.all_to_all(both.astype(BF), "y", 0, 0, tiled=True)
    return jnp.sum(pieces.astype(F32), axis=0).astype(BF)


def solution(mesh):
    finer = Mesh(mesh.devices.reshape(8, 4, 4, 2), ("z", "x", "y", "core"))
    sp, tp = ("z", "x"), ("y", "core")
    in_specs = (
        P(sp, None),
        P(),
        *(P(sp, tp) for _ in range(7)),
        P(None, tp),
        P(None, sp, tp),
        P(),
        P(None, tp),
        P(tp),
        P(tp, sp),
        P(tp, sp),
    )
    return jax.shard_map(
        on_device,
        mesh=finer,
        in_specs=in_specs,
        out_specs=P((*sp, *tp), None),
        check_vma=False,
    )
```

```python
import jax
import jax.numpy as jnp
from jax import lax
from jax.experimental import pallas as pl
from jax.experimental.pallas import tpu as pltpu
from jax.sharding import Mesh
from jax.sharding import PartitionSpec as P


CONV_KW = 31
BLOCK = 64
HEAD = 128
PACK = 144
BF = jnp.bfloat16
F32 = jnp.float32
SMEM = pl.BlockSpec(memory_space=pltpu.SMEM)
VMEM = pl.BlockSpec(memory_space=pltpu.VMEM)


def cost(micros):
    return pl.CostEstimate(flops=int(micros * 4e6), transcendentals=0, bytes_accessed=0)


def ring(count, step):
    return [(i, (i + step) % count) for i in range(count)]


def shift(array, axis, step):
    return lax.ppermute(array, axis, ring(lax.axis_size(axis), step))


def line(array, axes, step):
    count = lax.axis_size(axes)
    pairs = [(i, i + step) for i in range(count) if 0 <= i + step < count]
    return lax.ppermute(array, axes, pairs)


def ring_of_eight(block, axis):
    up, down = [block], [block]
    for _ in range(3):
        up.append(shift(up[-1], axis, 1))
        down.append(shift(down[-1], axis, -1))
    half = block.shape[0] // 2
    far = jnp.concatenate(
        [shift(up[3][:half], axis, 1), shift(down[3][half:], axis, -1)], axis=0
    )
    return [block, down[1], down[2], down[3], far, up[3], up[2], up[1]]


def ring_of_four(block, axis):
    ahead, behind = shift(block, axis, -1), shift(block, axis, 1)
    half = block.shape[0] // 2
    far = jnp.concatenate(
        [shift(behind[:half], axis, 1), shift(ahead[half:], axis, -1)], axis=0
    )
    return [block, ahead, far, behind]


def collect_kernel(a, b, c, d, e, f, g, rec, conv, first, later):
    for k, ref in enumerate((a, b, c)):
        first[:, k * HEAD : (k + 1) * HEAD] = ref[...]
    for k, ref in enumerate((d, e, f, g)):
        later[0, :, k * HEAD : (k + 1) * HEAD] = ref[...]
    later[0, :, 512:640] = rec[...].astype(F32).T.astype(BF)
    later[0, :, 640:768] = conv[...].astype(F32).T.astype(BF)
    for k in range(1, 8):
        later[k] = later[0]


def collected(*shards):
    return pl.pallas_call(
        collect_kernel,
        out_shape=(
            jax.ShapeDtypeStruct((64, 384), BF),
            jax.ShapeDtypeStruct((8, 64, 768), BF),
        ),
        cost_estimate=cost(2),
        name="collect",
    )(*shards)


def normalize_kernel(place, x, gain, out, other):
    z, turn = place[0], place[1]
    floats = x[...].astype(F32)
    factor = lax.rsqrt(jnp.mean(floats * floats, axis=-1, keepdims=True) + 1e-06)
    low = lax.broadcasted_iota(jnp.int32, (x.shape[0], HEAD), 1) < 64
    for pair in range(4):
        pieces = []
        for k in (2 * pair, 2 * pair + 1):
            at = slice(k * 256, (k + 1) * 256)
            scaled = x[:, at].astype(F32) * factor * gain[:, at].astype(F32)
            turned = pltpu.roll(scaled, turn, 1)
            to = pl.multiple_of(lax.rem(k + 8 - z, 8) * 256, 256)
            out[:, pl.ds(to, 256)] = turned.astype(BF)
            pieces.append((turned[:, :HEAD], turned[:, HEAD:]))
        for half in range(2):
            one, two = pieces[0][half], pieces[1][half]
            even = jnp.where(low, one, pltpu.roll(two, 64, 1))
            odd = jnp.where(low, pltpu.roll(one, 64, 1), two)
            for turn_at, value in ((2 * half, even), (2 * half + 1, odd)):
                at = turn_at * 512 + pair * HEAD
                other[:, at : at + HEAD] = value.astype(BF)


def normalized(x, gain, place):
    return pl.pallas_call(
        normalize_kernel,
        out_shape=(jax.ShapeDtypeStruct(x.shape, BF), jax.ShapeDtypeStruct(x.shape, BF)),
        in_specs=[SMEM, VMEM, VMEM],
        cost_estimate=cost(4),
        name="normalize",
    )(place, x, gain[None])


def nt(a, b):
    return lax.dot_general(a, b, (((1,), (1,)), ((), ())), preferred_element_type=F32)


def tn(a, b):
    return lax.dot_general(a, b, (((0,), (0,)), ((), ())), preferred_element_type=F32)


def pack(state, log):
    high = log.astype(BF).astype(F32)
    pad = jnp.zeros((PACK - HEAD - 8, HEAD), F32)
    rows = lax.broadcasted_iota(jnp.int32, (8, HEAD), 0)
    logs = jnp.where(rows == 0, high, jnp.where(rows == 1, log - high, 0.0))
    return jnp.concatenate([state, logs, pad], axis=0).astype(BF)


def unpack(message):
    state = message[:HEAD].astype(F32)
    logs = message[HEAD:PACK].astype(F32)
    return state, logs[0:1] + logs[1:2]


def gates_kernel(scores_f, scores_b, values, slack, extra, gap_o, cum_o, start_o, passed_o, send):
    length = values.shape[0]
    blocks = length // BLOCK
    inside = lax.rem(lax.broadcasted_iota(jnp.int32, (length, HEAD), 0), BLOCK)
    v = values[...].astype(BF)
    for d, scores in enumerate((scores_f, scores_b)):
        gap = slack[d : d + 1, :] * jax.nn.sigmoid(-scores[...])
        cum = jnp.log1p(-gap) + extra[d]
        step = 1
        while step < BLOCK:
            if d == 0:
                moved = jnp.where(inside >= step, pltpu.roll(cum, step, 0), 0.0)
            else:
                moved = jnp.where(inside < BLOCK - step, pltpu.roll(cum, length - step, 0), 0.0)
            cum = cum + moved
            step *= 2
        gap_o[d] = gap
        cum_o[d] = cum
        state = jnp.zeros((HEAD, HEAD), F32)
        passed = jnp.zeros((1, HEAD), F32)
        for n in range(blocks) if d == 0 else reversed(range(blocks)):
            rows = slice(n * BLOCK, (n + 1) * BLOCK)
            last = n * BLOCK + (BLOCK - 1 if d == 0 else 0)
            total = cum[last : last + 1]
            fade = gap[rows] * jnp.exp(total - cum[rows])
            start_o[d, n] = state.astype(BF)
            passed_o[d, n : n + 1] = passed
            state = jnp.exp(total) * state + tn(v[rows], fade.astype(BF))
            passed = passed + total
        message = pack(state, passed)
        for k in range(4):
            send[k, d] = message


def gates(scores_f, scores_b, values, slack, extra):
    length = values.shape[0]
    blocks = length // BLOCK
    return pl.pallas_call(
        gates_kernel,
        out_shape=(
            jax.ShapeDtypeStruct((2, length, HEAD), F32),
            jax.ShapeDtypeStruct((2, length, HEAD), F32),
            jax.ShapeDtypeStruct((2, blocks, HEAD, HEAD), BF),
            jax.ShapeDtypeStruct((2, 8, HEAD), F32),
            jax.ShapeDtypeStruct((4, 2, PACK, HEAD), BF),
        ),
        cost_estimate=cost(3),
        name="gates",
    )(scores_f, scores_b, values, slack, extra)


def row_kernel(place, got, before_o, send):
    x, z = place[2], place[0]
    messages = []
    for d in range(2):
        state = jnp.zeros((HEAD, HEAD), F32)
        log = jnp.zeros((1, HEAD), F32)
        before, passed = state, log
        for k in range(4) if d == 0 else reversed(range(4)):
            before = jnp.where(k == x, state, before)
            passed = jnp.where(k == x, log, passed)
            new, step = unpack(got[k, d])
            state = jnp.exp(step) * state + new
            log = log + step
        before_o[d, :HEAD] = before
        before_o[d, HEAD : HEAD + 8] = jnp.broadcast_to(passed, (8, HEAD))
        messages.append(pack(state, log))
    for k in range(8):
        send[k] = jnp.where(k > z, messages[0], messages[1])


def row_states(place, got):
    return pl.pallas_call(
        row_kernel,
        out_shape=(
            jax.ShapeDtypeStruct((2, HEAD + 8, HEAD), F32),
            jax.ShapeDtypeStruct((8, PACK, HEAD), BF),
        ),
        in_specs=[SMEM, VMEM],
        cost_estimate=cost(1),
        name="row",
    )(place, got)


def local_kernel(pre_query, values, gap, cum, start, passed, out, lifted_o):
    length = values.shape[0]
    blocks = length // BLOCK
    t = lax.broadcasted_iota(jnp.int32, (BLOCK, BLOCK), 0)
    s = lax.broadcasted_iota(jnp.int32, (BLOCK, BLOCK), 1)
    for n in range(blocks):
        rows = slice(n * BLOCK, (n + 1) * BLOCK)
        pre = pre_query[rows]
        q = pre * jax.nn.sigmoid(pre)
        v = values[rows].astype(BF)
        total = jnp.zeros((BLOCK, HEAD), F32)
        for d in range(2):
            c = cum[d, rows]
            lifted = q * jnp.exp(c)
            lowered = gap[d, rows] * jnp.exp(-c)
            scores = nt(lifted.astype(BF), lowered.astype(BF))
            scores = jnp.where(s <= t if d == 0 else s >= t, scores, 0.0)
            total = total + jnp.dot(scores.astype(BF), v, preferred_element_type=F32)
            total = total + nt(lifted.astype(BF), start[d, n])
            lifted_o[d, rows] = (lifted * jnp.exp(passed[d, n : n + 1])).astype(BF)
        out[rows] = total


def local_rows(pre_query, values, gap, cum, start, passed):
    length = values.shape[0]
    return pl.pallas_call(
        local_kernel,
        out_shape=(
            jax.ShapeDtypeStruct((length, HEAD), F32),
            jax.ShapeDtypeStruct((2, length, HEAD), BF),
        ),
        cost_estimate=cost(3),
        name="local",
    )(pre_query, values, gap, cum, start, passed)


def readout_kernel(place, local, lifted, every, before, rescale, out_gate, out):
    z = place[0]
    summed = local[...]
    for d in range(2):
        state = jnp.zeros((HEAD, HEAD), F32)
        for k in range(8) if d == 0 else reversed(range(8)):
            new, step = unpack(every[k])
            state = jnp.where(k < z if d == 0 else k > z, jnp.exp(step) * state + new, state)
        incoming = before[d, :HEAD] + jnp.exp(before[d, HEAD : HEAD + 1]) * state
        summed = summed + nt(lifted[d], incoming.astype(BF))
    factor = lax.rsqrt(jnp.mean(summed * summed, axis=-1, keepdims=True) + 1e-06)
    gate = out_gate[...]
    scaled = summed * factor * rescale[...].astype(F32)
    out[...] = (scaled * (gate * jax.nn.sigmoid(gate))).astype(BF)


def readout(place, local, lifted, every, before, rescale, out_gate):
    return pl.pallas_call(
        readout_kernel,
        out_shape=jax.ShapeDtypeStruct(local.shape, BF),
        in_specs=[SMEM, *[VMEM] * 6],
        cost_estimate=cost(2),
        name="readout",
    )(place, local, lifted, every, before, rescale[None], out_gate)


def columns_kernel(place, a, b, c, d, out):
    x = place[2]
    for k, piece in enumerate((a, b, c, d)):
        turn = lax.rem(x + k, 4)
        for z in range(8):
            to = pl.multiple_of((z * 4 + turn) * 64, 64)
            out[pl.ds(to, 64)] = piece[z * 64 : (z + 1) * 64, 512:768]


def columns_in_order(place, pieces):
    return pl.pallas_call(
        columns_kernel,
        out_shape=jax.ShapeDtypeStruct((2048, 256), BF),
        in_specs=[SMEM, *[VMEM] * 4],
        cost_estimate=cost(1),
        name="columns",
    )(place, *pieces)


def project_out_kernel(place, rec, conv, columns, out):
    core = place[0]
    for k in range(4):
        at = pl.multiple_of(k * 96 + core * 48, 16)
        part = nt(rec[pl.ds(at, 48)], columns[:, :HEAD])
        part = part + nt(conv[pl.ds(at, 48)], columns[:, HEAD:])
        out[k] = part.astype(out.dtype)


def project_out(core, rec, conv, columns, kind):
    return pl.pallas_call(
        project_out_kernel,
        out_shape=jax.ShapeDtypeStruct((4, 48, 2048), kind),
        in_specs=[SMEM, VMEM, VMEM, VMEM],
        cost_estimate=cost(2),
        name="project_out",
    )(core, rec, conv, columns)


def meet_kernel(place, mine, got, far_low, far_high, ahead, behind, own):
    y = place[3]

    def block(step):
        k = lax.rem(y + step, 4)
        return mine[k] + got[k].astype(F32)

    far = block(2)
    far_low[...] = far[:, :1024].astype(BF)
    far_high[...] = far[:, 1024:].astype(BF)
    ahead[...] = block(1)
    behind[...] = block(3)
    own[...] = block(0)


def meet(place, mine, got):
    half = jax.ShapeDtypeStruct((48, 1024), BF)
    whole = jax.ShapeDtypeStruct((48, 2048), F32)
    return pl.pallas_call(
        meet_kernel,
        out_shape=(half, half, whole, whole, whole),
        in_specs=[SMEM, VMEM, VMEM],
        cost_estimate=cost(1),
        name="meet",
    )(place, mine, got)


def relay_kernel(ahead, behind, low, high, ahead_o, behind_o):
    ahead_o[:, :1024] = (ahead[:, :1024] + low[...].astype(F32)).astype(BF)
    ahead_o[:, 1024:] = ahead[:, 1024:].astype(BF)
    behind_o[:, :1024] = behind[:, :1024].astype(BF)
    behind_o[:, 1024:] = (behind[:, 1024:] + high[...].astype(F32)).astype(BF)


def relay(ahead, behind, low, high):
    whole = jax.ShapeDtypeStruct((48, 2048), BF)
    return pl.pallas_call(
        relay_kernel, out_shape=(whole, whole), cost_estimate=cost(0.5), name="relay"
    )(ahead, behind, low, high)


def depthwise(framed, filter_kernel_coefs):
    channels = framed.shape[1]
    result = lax.conv_general_dilated(
        framed[None],
        filter_kernel_coefs[:, None, :],
        (1,),
        "VALID",
        dimension_numbers=("NWC", "WIO", "NWC"),
        feature_group_count=channels,
        preferred_element_type=F32,
    )
    return result[0]


def group_norm_silu(conv_sum, channel_cluster_scale):
    centred = conv_sum - jnp.mean(conv_sum, axis=-1, keepdims=True)
    variance = jnp.mean(centred * centred, axis=-1, keepdims=True)
    standard = centred * lax.rsqrt(variance + 1e-05)
    return jax.nn.silu(standard * channel_cluster_scale.astype(F32)).astype(BF)


def project(rows, blocks):
    total, at = None, 0
    for block in blocks:
        part = jnp.dot(
            rows[:, at : at + block.shape[0]], block, preferred_element_type=F32
        )
        at += block.shape[0]
        total = part if total is None else total + part
    return total


def on_device(
    sequence_embeddings,
    entry_rescale_vector,
    probe_matrix,
    onward_retain_matrix,
    reverse_retain_matrix,
    content_matrix,
    emission_switch_matrix,
    pointwise_content_matrix,
    pointwise_switch_matrix,
    retain_lower_slack,
    extra_log_shrink,
    subspace_rescale,
    filter_kernel_coefs,
    channel_cluster_scale,
    scan_readout_matrix,
    filter_readout_matrix,
):
    x, z, y = (lax.axis_index(axis) for axis in "xzy")
    core = lax.axis_index("core")
    place = jnp.stack([z, lax.rem(4 - x, 4) * 64, x, y]).astype(jnp.int32)
    first, later = collected(
        onward_retain_matrix,
        reverse_retain_matrix,
        content_matrix,
        probe_matrix,
        emission_switch_matrix,
        pointwise_content_matrix,
        pointwise_switch_matrix,
        scan_readout_matrix,
        filter_readout_matrix,
    )
    later = lax.all_to_all(later, "z", 0, 0, tiled=True).reshape(512, 768)
    near = jnp.concatenate(
        [first, shift(first, "x", -1), shift(first, "x", 2), shift(first, "x", 1)], axis=0
    )
    normed, normed_later = normalized(sequence_embeddings, entry_rescale_vector, place)
    near, normed, normed_later = lax.optimization_barrier((near, normed, normed_later))
    scores = project(normed, ring_of_eight(near, "z"))
    later_blocks = ring_of_four(later, "x")

    values = scores[:, 256:384]
    gap, cum, start, passed, send = gates(
        scores[:, :128], scores[:, 128:256], values, retain_lower_slack, extra_log_shrink
    )
    got = lax.all_to_all(send, "x", 0, 0, tiled=True)
    before, send = row_states(place, got)
    every = lax.all_to_all(send, "z", 0, 0, tiled=True)

    later_scores = project(normed_later, [block[:, :512] for block in later_blocks])
    pre_query, out_gate, glu_a, glu_b = (later_scores[:, k * 128 : (k + 1) * 128] for k in range(4))
    glu = (glu_a * jax.nn.sigmoid(glu_b)).astype(BF)
    reach = CONV_KW // 2
    low = line(glu[-reach:], ("z", "x"), 1)
    high = line(glu[:reach], ("z", "x"), -1)
    framed = jnp.concatenate([low, glu, high], axis=0)
    conv_out = group_norm_silu(depthwise(framed, filter_kernel_coefs), channel_cluster_scale)
    columns = columns_in_order(place, later_blocks)
    local, lifted = local_rows(pre_query, values, gap, cum, start, passed)
    rec_out = readout(place, local, lifted, every, before, subspace_rescale, out_gate)

    theirs = project_out((1 - core)[None], rec_out, conv_out, columns, BF)
    mine = project_out(core[None], rec_out, conv_out, columns, F32)
    far_low, far_high, ahead, behind, own = meet(place, mine, shift(theirs, "core", 1))
    ahead, behind = relay(ahead, behind, shift(far_low, "y", 1), shift(far_high, "y", -1))
    ahead, behind = shift(ahead, "y", 1), shift(behind, "y", -1)
    return (own + ahead.astype(F32) + behind.astype(F32)).astype(BF)


def solution(mesh):
    finer = Mesh(mesh.devices.reshape(8, 4, 4, 2), ("z", "x", "y", "core"))
    sp, tp = ("z", "x"), ("y", "core")
    in_specs = (
        P(sp, None),
        P(),
        *(P(sp, tp) for _ in range(7)),
        P(None, tp),
        P(None, sp, tp),
        P(),
        P(None, tp),
        P(tp),
        P(tp, sp),
        P(tp, sp),
    )
    return jax.shard_map(
        on_device,
        mesh=finer,
        in_specs=in_specs,
        out_specs=P((*sp, *tp), None),
        check_vma=False,
    )
```

```python
import jax
import jax.numpy as jnp
from jax import lax
from jax.experimental import pallas as pl
from jax.experimental.pallas import tpu as pltpu
from jax.sharding import Mesh
from jax.sharding import PartitionSpec as P


CONV_KW = 31
BLOCK = 64
HEAD = 128
PACK = 144
BF = jnp.bfloat16
F32 = jnp.float32
ROOM = pltpu.CompilerParams(vmem_limit_bytes=24 * 2**20)
SMEM = pl.BlockSpec(memory_space=pltpu.SMEM)
VMEM = pl.BlockSpec(memory_space=pltpu.VMEM)


def ring(count, step):
    return [(i, (i + step) % count) for i in range(count)]


def shift(array, axis, step):
    return lax.ppermute(array, axis, ring(lax.axis_size(axis), step))


def line(array, axes, step):
    count = lax.axis_size(axes)
    pairs = [(i, i + step) for i in range(count) if 0 <= i + step < count]
    return lax.ppermute(array, axes, pairs)


def ring_of_eight(block, axis):
    up, down = [block], [block]
    for _ in range(3):
        up.append(shift(up[-1], axis, 1))
        down.append(shift(down[-1], axis, -1))
    half = block.shape[0] // 2
    far = jnp.concatenate(
        [shift(up[3][:half], axis, 1), shift(down[3][half:], axis, -1)], axis=0
    )
    return [block, down[1], down[2], down[3], far, up[3], up[2], up[1]]


def keep(array):
    return pltpu.with_memory_space_constraint(array, pltpu.VMEM)


def far_off(array):
    return pltpu.with_memory_space_constraint(array, pltpu.HBM)


def kernel_call(body, name, micros, outs, *operands, scratch=()):
    return pl.pallas_call(
        body,
        out_shape=tuple(outs),
        in_specs=[SMEM if o.dtype == jnp.int32 else VMEM for o in operands],
        scratch_shapes=list(scratch),
        compiler_params=ROOM,
        cost_estimate=pl.CostEstimate(
            flops=int(micros * 4e6), transcendentals=0, bytes_accessed=0
        ),
        name=name,
    )(*operands)


def nt(a, b):
    return lax.dot_general(a, b, (((1,), (1,)), ((), ())), preferred_element_type=F32)


def tn(a, b):
    return lax.dot_general(a, b, (((0,), (0,)), ((), ())), preferred_element_type=F32)


def dot(a, b):
    return jnp.dot(a, b, preferred_element_type=F32)


def collect_kernel(*refs):
    out = refs[-1]
    at = 0
    for ref in refs[:-1]:
        out[:, at : at + HEAD] = ref[...]
        at += HEAD


def stack_kernel(own, ahead, far, behind, first, later):
    for k, ref in enumerate((own, ahead, far, behind)):
        rows = slice(k * 64, (k + 1) * 64)
        first[rows] = ref[:, :384]
        later[rows] = ref[:, 384:]


def normalize_kernel(place, x, gain, out):
    turn = place[1]
    floats = x[...].astype(F32)
    factor = lax.rsqrt(jnp.mean(floats * floats, axis=-1, keepdims=True) + 1e-06)
    for k in range(8):
        at = slice(k * 256, (k + 1) * 256)
        scaled = x[:, at].astype(F32) * factor * gain[:, at].astype(F32)
        out[:, at] = pltpu.roll(scaled, turn, 1).astype(BF)


def normalized(place, x, gain):
    (out,) = kernel_call(normalize_kernel, "normalize", 3, [pltpu.VMEM(x.shape, BF)], place, x, gain)
    return out


def near_scores_kernel(place, normed, own, a1, b1, a2, b2, out):
    z = place[0]
    total = None
    for step, block in ((0, own), (1, a1), (7, b1), (2, a2), (6, b2)):
        at = pl.multiple_of(lax.rem(z + step, 8) * 256, 256)
        part = dot(normed[:, pl.ds(at, 256)], block[...])
        total = part if total is None else total + part
    out[...] = total


def pack(state, log):
    high = log.astype(BF).astype(F32)
    pad = jnp.zeros((PACK - HEAD - 8, HEAD), F32)
    rows = lax.broadcasted_iota(jnp.int32, (8, HEAD), 0)
    logs = jnp.where(rows == 0, high, jnp.where(rows == 1, log - high, 0.0))
    return jnp.concatenate([state, logs, pad], axis=0).astype(BF)


def unpack(message):
    state = message[:HEAD].astype(F32)
    logs = message[HEAD:PACK].astype(F32)
    return state, logs[0:1] + logs[1:2]


def gates_kernel(place, near, normed, a3, far, b3, slack, extra, values_o, gap_o, cum_o, start_o, passed_o, send):
    z = place[0]
    length = near.shape[0]
    blocks = length // BLOCK
    scores = near[...]
    for step, block in ((3, a3), (4, far), (5, b3)):
        at = pl.multiple_of(lax.rem(z + step, 8) * 256, 256)
        scores = scores + dot(normed[:, pl.ds(at, 256)], block[...])
    inside = lax.rem(lax.broadcasted_iota(jnp.int32, (length, HEAD), 0), BLOCK)
    v = scores[:, 256:].astype(BF)
    values_o[...] = v
    for d in range(2):
        gap = slack[d : d + 1, :] * jax.nn.sigmoid(-scores[:, d * HEAD : (d + 1) * HEAD])
        cum = jnp.log1p(-gap) + extra[d]
        step = 1
        while step < BLOCK:
            if d == 0:
                moved = jnp.where(inside >= step, pltpu.roll(cum, step, 0), 0.0)
            else:
                moved = jnp.where(inside < BLOCK - step, pltpu.roll(cum, length - step, 0), 0.0)
            cum = cum + moved
            step *= 2
        gap_o[d] = gap
        cum_o[d] = cum
        state = jnp.zeros((HEAD, HEAD), F32)
        passed = jnp.zeros((1, HEAD), F32)
        for n in range(blocks) if d == 0 else reversed(range(blocks)):
            rows = slice(n * BLOCK, (n + 1) * BLOCK)
            last = n * BLOCK + (BLOCK - 1 if d == 0 else 0)
            total = cum[last : last + 1]
            fade = gap[rows] * jnp.exp(total - cum[rows])
            start_o[d, n] = state.astype(BF)
            passed_o[d, n : n + 1] = passed
            state = jnp.exp(total) * state + tn(v[rows], fade.astype(BF))
            passed = passed + total
        message = pack(state, passed)
        for k in range(4):
            send[k, d] = message


def row_kernel(place, got, before_o, send):
    x, z = place[2], place[0]
    messages = []
    for d in range(2):
        state = jnp.zeros((HEAD, HEAD), F32)
        log = jnp.zeros((1, HEAD), F32)
        before, passed = state, log
        for k in range(4) if d == 0 else reversed(range(4)):
            before = jnp.where(k == x, state, before)
            passed = jnp.where(k == x, log, passed)
            new, step = unpack(got[k, d])
            state = jnp.exp(step) * state + new
            log = log + step
        before_o[d, :HEAD] = before
        before_o[d, HEAD : HEAD + 8] = jnp.broadcast_to(passed, (8, HEAD))
        messages.append(pack(state, log))
    for k in range(8):
        send[k] = jnp.where(k > z, messages[0], messages[1])


def later_kernel(place, normed, edges, weights, values, gap, cum, start, passed, taps, scale, local_o, lifted_o, gate_o, conv_o, columns_o, query, glu):
    x = place[2]
    length = normed.shape[0]
    blocks = length // BLOCK
    pre = dot(normed[...], weights[:, :256])
    query[...] = pre[:, :HEAD] * jax.nn.sigmoid(pre[:, :HEAD])
    gate_o[...] = pre[:, HEAD:] * jax.nn.sigmoid(pre[:, HEAD:])

    def gated(rows):
        pair = dot(rows, weights[:, 256:512])
        return (pair[:, :HEAD] * jax.nn.sigmoid(pair[:, HEAD:])).astype(BF).astype(F32)

    glu[16 : 16 + length] = gated(normed[...])
    edge = gated(edges[...])
    glu[:16] = edge[:16]
    glu[16 + length :] = edge[16:]
    framed = glu[...]
    kernel = taps[...].astype(F32)
    total = None
    for r in range(8):
        turned = framed if r == 0 else pltpu.roll(framed, length + 32 - r, 0)
        for j in range(CONV_KW):
            if (1 + j) % 8 == r:
                at = (1 + j) - r
                part = turned[at : at + length] * kernel[j : j + 1]
                total = part if total is None else total + part
    centred = total - jnp.mean(total, axis=-1, keepdims=True)
    variance = jnp.mean(centred * centred, axis=-1, keepdims=True)
    standard = centred * lax.rsqrt(variance + 1e-05) * scale[...].astype(F32)
    conv_o[...] = (standard * jax.nn.sigmoid(standard)).astype(BF)

    for k in range(4):
        turn = lax.rem(x + k, 4)
        for z in range(8):
            to = pl.multiple_of((z * 4 + turn) * 64, 64)
            at = (z * 4 + k) * 64
            columns_o[pl.ds(to, 64)] = weights[at : at + 64, 512:768]

    t = lax.broadcasted_iota(jnp.int32, (BLOCK, BLOCK), 0)
    s = lax.broadcasted_iota(jnp.int32, (BLOCK, BLOCK), 1)
    for n in range(blocks):
        rows = slice(n * BLOCK, (n + 1) * BLOCK)
        q = query[rows]
        v = values[rows]
        total = jnp.zeros((BLOCK, HEAD), F32)
        for d in range(2):
            c = cum[d, rows]
            lifted = q * jnp.exp(c)
            lowered = gap[d, rows] * jnp.exp(-c)
            scores = nt(lifted.astype(BF), lowered.astype(BF))
            scores = jnp.where(s <= t if d == 0 else s >= t, scores, 0.0)
            total = total + dot(scores.astype(BF), v)
            total = total + nt(lifted.astype(BF), start[d, n])
            lifted_o[d, rows] = (lifted * jnp.exp(passed[d, n : n + 1])).astype(BF)
        local_o[rows] = total


def readout_kernel(place, local, lifted, every, before, rescale, gate, out):
    z = place[0]
    summed = local[...]
    for d in range(2):
        state = jnp.zeros((HEAD, HEAD), F32)
        for k in range(8) if d == 0 else reversed(range(8)):
            new, step = unpack(every[k])
            state = jnp.where(k < z if d == 0 else k > z, jnp.exp(step) * state + new, state)
        incoming = before[d, :HEAD] + jnp.exp(before[d, HEAD : HEAD + 1]) * state
        summed = summed + nt(lifted[d], incoming.astype(BF))
    factor = lax.rsqrt(jnp.mean(summed * summed, axis=-1, keepdims=True) + 1e-06)
    out[...] = (summed * factor * rescale[...].astype(F32) * gate[...]).astype(BF)


def project_out_kernel(place, rec, conv, columns, out):
    core = place[0]
    at = [pl.multiple_of(k * 96 + core * 48, 16) for k in range(4)]
    left = jnp.concatenate([rec[pl.ds(k, 48)] for k in at], axis=0)
    right = jnp.concatenate([conv[pl.ds(k, 48)] for k in at], axis=0)
    rows = jnp.concatenate([left, right], axis=1)
    for c in range(0, 2048, 512):
        part = nt(rows, columns[c : c + 512])
        for k in range(4):
            out[k, :, c : c + 512] = part[k * 48 : (k + 1) * 48].astype(out.dtype)


def meet_kernel(place, mine, got, far_low, far_high, ahead, behind, own):
    y = place[3]

    def block(step):
        k = lax.rem(y + step, 4)
        return mine[k] + got[k].astype(F32)

    far = block(2)
    far_low[...] = far[:, :1024].astype(BF)
    far_high[...] = far[:, 1024:].astype(BF)
    ahead[...] = block(1)
    behind[...] = block(3)
    own[...] = block(0)


def relay_kernel(ahead, behind, low, high, ahead_o, behind_o):
    ahead_o[:, :1024] = (ahead[:, :1024] + low[...].astype(F32)).astype(BF)
    ahead_o[:, 1024:] = ahead[:, 1024:].astype(BF)
    behind_o[:, :1024] = behind[:, :1024].astype(BF)
    behind_o[:, 1024:] = (behind[:, 1024:] + high[...].astype(F32)).astype(BF)


def on_device(
    sequence_embeddings,
    entry_rescale_vector,
    probe_matrix,
    onward_retain_matrix,
    reverse_retain_matrix,
    content_matrix,
    emission_switch_matrix,
    pointwise_content_matrix,
    pointwise_switch_matrix,
    retain_lower_slack,
    extra_log_shrink,
    subspace_rescale,
    filter_kernel_coefs,
    channel_cluster_scale,
    scan_readout_matrix,
    filter_readout_matrix,
):
    x, z, y = (lax.axis_index(axis) for axis in "xzy")
    core = lax.axis_index("core")
    length = sequence_embeddings.shape[0]
    gain = entry_rescale_vector[None]
    place = jnp.stack([z, lax.rem(4 - x, 4) * 64, x, y]).astype(jnp.int32)
    (shard,) = kernel_call(
        collect_kernel,
        "collect",
        2,
        [pltpu.VMEM((64, 1152), BF)],
        *(
            far_off(weight)
            for weight in (
                onward_retain_matrix,
                reverse_retain_matrix,
                content_matrix,
                probe_matrix,
                emission_switch_matrix,
                pointwise_content_matrix,
                pointwise_switch_matrix,
                scan_readout_matrix.T,
                filter_readout_matrix.T,
            )
        ),
    )
    ahead, far, behind = shift(shard, "x", -1), shift(shard, "x", 2), shift(shard, "x", 1)
    normed = normalized(place, far_off(sequence_embeddings), gain)
    normed, shard, ahead, far, behind = lax.optimization_barrier(
        (normed, shard, ahead, far, behind)
    )
    first, later = kernel_call(
        stack_kernel,
        "stack",
        1,
        [pltpu.VMEM((256, 384), BF), pltpu.HBM((256, 768), BF)],
        keep(shard),
        keep(ahead),
        keep(far),
        keep(behind),
    )
    weights = lax.all_gather(later, "z", axis=0, tiled=True)
    edges = jnp.concatenate(
        [
            line(sequence_embeddings[-16:], ("z", "x"), 1),
            line(sequence_embeddings[:16], ("z", "x"), -1),
        ],
        axis=0,
    )
    edges = normalized(place, edges, gain)
    own, a1, a2, a3, far, b3, b2, b1 = (keep(block) for block in ring_of_eight(first, "z"))
    normed = keep(normed)
    (near,) = kernel_call(
        near_scores_kernel,
        "near",
        1,
        [pltpu.VMEM((length, 384), F32)],
        place,
        normed,
        own,
        a1,
        b1,
        a2,
        b2,
    )
    blocks = length // BLOCK
    values, gap, cum, start, passed, send = kernel_call(
        gates_kernel,
        "gates",
        3,
        [
            pltpu.HBM((length, HEAD), BF),
            pltpu.HBM((2, length, HEAD), F32),
            pltpu.HBM((2, length, HEAD), F32),
            pltpu.HBM((2, blocks, HEAD, HEAD), BF),
            pltpu.HBM((2, 8, HEAD), F32),
            pltpu.VMEM((4, 2, PACK, HEAD), BF),
        ],
        place,
        keep(near),
        normed,
        a3,
        far,
        b3,
        retain_lower_slack,
        extra_log_shrink,
    )
    got = lax.all_to_all(send, "x", 0, 0, tiled=True)
    before, send = kernel_call(
        row_kernel,
        "row",
        1,
        [pltpu.HBM((2, HEAD + 8, HEAD), F32), pltpu.VMEM((8, PACK, HEAD), BF)],
        place,
        keep(got),
    )
    every = lax.all_to_all(send, "z", 0, 0, tiled=True)

    local, lifted, gate, conv_out, columns = kernel_call(
        later_kernel,
        "later",
        6,
        [
            pltpu.HBM((length, HEAD), F32),
            pltpu.HBM((2, length, HEAD), BF),
            pltpu.HBM((length, HEAD), F32),
            pltpu.VMEM((length, HEAD), BF),
            pltpu.VMEM((2048, 256), BF),
        ],
        place,
        normed,
        keep(edges),
        *(far_off(a) for a in (weights, values, gap, cum, start, passed)),
        filter_kernel_coefs,
        channel_cluster_scale[None],
        scratch=(pltpu.VMEM((length, HEAD), F32), pltpu.VMEM((length + 32, HEAD), F32)),
    )
    (rec_out,) = kernel_call(
        readout_kernel,
        "readout",
        1,
        [pltpu.VMEM((length, HEAD), BF)],
        place,
        far_off(local),
        far_off(lifted),
        keep(every),
        far_off(before),
        subspace_rescale[None],
        far_off(gate),
    )
    theirs, mine = (
        kernel_call(
            project_out_kernel,
            "project_out",
            1,
            [pltpu.VMEM((4, 48, 2048), kind)],
            side[None].astype(jnp.int32),
            keep(rec_out),
            keep(conv_out),
            keep(columns),
        )[0]
        for side, kind in ((1 - core, BF), (core, F32))
    )
    half, whole, final = (
        pltpu.VMEM((48, 1024), BF),
        pltpu.VMEM((48, 2048), F32),
        pltpu.VMEM((48, 2048), BF),
    )
    far_low, far_high, ahead, behind, own = kernel_call(
        meet_kernel,
        "meet",
        1,
        [half, half, whole, whole, whole],
        place,
        keep(mine),
        keep(shift(theirs, "core", 1)),
    )
    ahead, behind = kernel_call(
        relay_kernel,
        "relay",
        0.5,
        [final, final],
        keep(ahead),
        keep(behind),
        keep(shift(far_low, "y", 1)),
        keep(shift(far_high, "y", -1)),
    )
    ahead, behind = shift(ahead, "y", 1), shift(behind, "y", -1)
    return (own + ahead.astype(F32) + behind.astype(F32)).astype(BF)


def solution(mesh):
    finer = Mesh(mesh.devices.reshape(8, 4, 4, 2), ("z", "x", "y", "core"))
    sp, tp = ("z", "x"), ("y", "core")
    in_specs = (
        P(sp, None),
        P(),
        *(P(sp, tp) for _ in range(7)),
        P(None, tp),
        P(None, sp, tp),
        P(),
        P(None, tp),
        P(tp),
        P(tp, sp),
        P(tp, sp),
    )
    return jax.shard_map(
        on_device,
        mesh=finer,
        in_specs=in_specs,
        out_specs=P((*sp, *tp), None),
        check_vma=False,
    )
```

```python
import jax
import jax.numpy as jnp
from jax import lax
from jax.experimental import pallas as pl
from jax.experimental.pallas import tpu as pltpu
from jax.sharding import Mesh
from jax.sharding import PartitionSpec as P


CONV_KW = 31
BLOCK = 64
HEAD = 128
PACK = 144
BF = jnp.bfloat16
F32 = jnp.float32
ROOM = pltpu.CompilerParams(vmem_limit_bytes=24 * 2**20)
SMEM = pl.BlockSpec(memory_space=pltpu.SMEM)
VMEM = pl.BlockSpec(memory_space=pltpu.VMEM)


def ring(count, step):
    return [(i, (i + step) % count) for i in range(count)]


def shift(array, axis, step):
    return lax.ppermute(array, axis, ring(lax.axis_size(axis), step))


def line(array, axes, step):
    count = lax.axis_size(axes)
    pairs = [(i, i + step) for i in range(count) if 0 <= i + step < count]
    return lax.ppermute(array, axes, pairs)


def keep(array):
    return pltpu.with_memory_space_constraint(array, pltpu.VMEM)


def far_off(array):
    return pltpu.with_memory_space_constraint(array, pltpu.HBM)


def kernel_call(body, name, micros, outs, *operands, scratch=()):
    return pl.pallas_call(
        body,
        out_shape=tuple(outs),
        in_specs=[SMEM if o.dtype == jnp.int32 else VMEM for o in operands],
        scratch_shapes=list(scratch),
        compiler_params=ROOM,
        cost_estimate=pl.CostEstimate(
            flops=int(micros * 4e6), transcendentals=0, bytes_accessed=0
        ),
        name=name,
    )(*operands)


def nt(a, b):
    return lax.dot_general(a, b, (((1,), (1,)), ((), ())), preferred_element_type=F32)


def tn(a, b):
    return lax.dot_general(a, b, (((0,), (0,)), ((), ())), preferred_element_type=F32)


def dot(a, b):
    return jnp.dot(a, b, preferred_element_type=F32)


def collect_kernel(*refs):
    first, later = refs[-2:]
    for k, ref in enumerate(refs[:3]):
        for z in range(8):
            first[z, :, k * HEAD : (k + 1) * HEAD] = ref[...]
    for k, ref in enumerate(refs[3:-2]):
        later[:, k * HEAD : (k + 1) * HEAD] = ref[...]


def stack_kernel(own, ahead, far, behind, later):
    for k, ref in enumerate((own, ahead, far, behind)):
        later[k * 64 : (k + 1) * 64] = ref[...]


def normalize_kernel(place, x, gain, out, *other):
    turn = place[1]
    floats = x[...].astype(F32)
    factor = lax.rsqrt(jnp.mean(floats * floats, axis=-1, keepdims=True) + 1e-06)
    low = lax.broadcasted_iota(jnp.int32, (x.shape[0], HEAD), 1) < 64
    for pair in range(4):
        pieces = []
        for k in (2 * pair, 2 * pair + 1):
            at = slice(k * 256, (k + 1) * 256)
            scaled = x[:, at].astype(F32) * factor * gain[:, at].astype(F32)
            turned = pltpu.roll(scaled, turn, 1)
            out[:, at] = turned.astype(BF)
            pieces.append((turned[:, :HEAD], turned[:, HEAD:]))
        if other:
            for half in range(2):
                one, two = pieces[0][half], pieces[1][half]
                even = jnp.where(low, one, pltpu.roll(two, 64, 1))
                odd = jnp.where(low, pltpu.roll(one, 64, 1), two)
                for piece, value in ((2 * half, even), (2 * half + 1, odd)):
                    at = piece * 512 + pair * HEAD
                    other[0][:, at : at + HEAD] = value.astype(BF)


def normalized(place, x, gain, count):
    outs = [pltpu.VMEM(x.shape, BF)] * count
    return kernel_call(normalize_kernel, "normalize", 3, outs, place, x, gain)


def near_scores_kernel(normed, own, ahead, behind, out):
    total = dot(normed[:, :512], own[...])
    total = total + dot(normed[:, 512:1024], ahead[...])
    out[...] = total + dot(normed[:, 1536:], behind[...])


def pack(state, log):
    high = log.astype(BF).astype(F32)
    pad = jnp.zeros((PACK - HEAD - 8, HEAD), F32)
    rows = lax.broadcasted_iota(jnp.int32, (8, HEAD), 0)
    logs = jnp.where(rows == 0, high, jnp.where(rows == 1, log - high, 0.0))
    return jnp.concatenate([state, logs, pad], axis=0).astype(BF)


def unpack(message):
    state = message[:HEAD].astype(F32)
    logs = message[HEAD:PACK].astype(F32)
    return state, logs[0:1] + logs[1:2]


def gates_kernel(near, normed, far_low, far_high, slack, extra, values_o, gap_o, cum_o, start_o, passed_o, send):
    length = near.shape[0]
    blocks = length // BLOCK
    scores = near[...] + dot(normed[:, 1024:1280], far_low[...])
    scores = scores + dot(normed[:, 1280:1536], far_high[...])
    inside = lax.rem(lax.broadcasted_iota(jnp.int32, (length, HEAD), 0), BLOCK)
    v = scores[:, 256:].astype(BF)
    values_o[...] = v
    for d in range(2):
        gap = slack[d : d + 1, :] * jax.nn.sigmoid(-scores[:, d * HEAD : (d + 1) * HEAD])
        cum = jnp.log1p(-gap) + extra[d]
        step = 1
        while step < BLOCK:
            if d == 0:
                moved = jnp.where(inside >= step, pltpu.roll(cum, step, 0), 0.0)
            else:
                moved = jnp.where(inside < BLOCK - step, pltpu.roll(cum, length - step, 0), 0.0)
            cum = cum + moved
            step *= 2
        gap_o[d] = gap
        cum_o[d] = cum
        state = jnp.zeros((HEAD, HEAD), F32)
        passed = jnp.zeros((1, HEAD), F32)
        for n in range(blocks) if d == 0 else reversed(range(blocks)):
            rows = slice(n * BLOCK, (n + 1) * BLOCK)
            last = n * BLOCK + (BLOCK - 1 if d == 0 else 0)
            total = cum[last : last + 1]
            fade = gap[rows] * jnp.exp(total - cum[rows])
            start_o[d, n] = state.astype(BF)
            passed_o[d, n : n + 1] = passed
            state = jnp.exp(total) * state + tn(v[rows], fade.astype(BF))
            passed = passed + total
        message = pack(state, passed)
        for k in range(4):
            send[k, d] = message


def row_kernel(place, got, before_o, send):
    x, z = place[2], place[0]
    messages = []
    for d in range(2):
        state = jnp.zeros((HEAD, HEAD), F32)
        log = jnp.zeros((1, HEAD), F32)
        before, passed = state, log
        for k in range(4) if d == 0 else reversed(range(4)):
            before = jnp.where(k == x, state, before)
            passed = jnp.where(k == x, log, passed)
            new, step = unpack(got[k, d])
            state = jnp.exp(step) * state + new
            log = log + step
        before_o[d, :HEAD] = before
        before_o[d, HEAD : HEAD + 8] = jnp.broadcast_to(passed, (8, HEAD))
        messages.append(pack(state, log))
    for k in range(8):
        send[k] = jnp.where(k > z, messages[0], messages[1])


def later_kernel(place, normed, edges, weights, values, gap, cum, start, passed, taps, scale, local_o, lifted_o, gate_o, conv_o, columns_o, query, glu):
    x = place[2]
    length = normed.shape[0]
    blocks = length // BLOCK
    pre = dot(normed[...], weights[:, :256])
    query[...] = pre[:, :HEAD] * jax.nn.sigmoid(pre[:, :HEAD])
    gate_o[...] = pre[:, HEAD:] * jax.nn.sigmoid(pre[:, HEAD:])

    def gated(rows):
        pair = dot(rows, weights[:, 256:512])
        return (pair[:, :HEAD] * jax.nn.sigmoid(pair[:, HEAD:])).astype(BF).astype(F32)

    glu[16 : 16 + length] = gated(normed[...])
    edge = gated(edges[...])
    glu[:16] = edge[:16]
    glu[16 + length :] = edge[16:]
    framed = glu[...]
    kernel = taps[...].astype(F32)
    total = None
    for r in range(8):
        turned = framed if r == 0 else pltpu.roll(framed, length + 32 - r, 0)
        for j in range(CONV_KW):
            if (1 + j) % 8 == r:
                at = (1 + j) - r
                part = turned[at : at + length] * kernel[j : j + 1]
                total = part if total is None else total + part
    centred = total - jnp.mean(total, axis=-1, keepdims=True)
    variance = jnp.mean(centred * centred, axis=-1, keepdims=True)
    standard = centred * lax.rsqrt(variance + 1e-05) * scale[...].astype(F32)
    conv_o[...] = (standard * jax.nn.sigmoid(standard)).astype(BF)

    for k in range(4):
        turn = lax.rem(x + k, 4)
        for z in range(8):
            to = pl.multiple_of((z * 4 + turn) * 64, 64)
            at = (z * 4 + k) * 64
            columns_o[pl.ds(to, 64)] = weights[at : at + 64, 512:768]

    t = lax.broadcasted_iota(jnp.int32, (BLOCK, BLOCK), 0)
    s = lax.broadcasted_iota(jnp.int32, (BLOCK, BLOCK), 1)
    for n in range(blocks):
        rows = slice(n * BLOCK, (n + 1) * BLOCK)
        q = query[rows]
        v = values[rows]
        total = jnp.zeros((BLOCK, HEAD), F32)
        for d in range(2):
            c = cum[d, rows]
            lifted = q * jnp.exp(c)
            lowered = gap[d, rows] * jnp.exp(-c)
            scores = nt(lifted.astype(BF), lowered.astype(BF))
            scores = jnp.where(s <= t if d == 0 else s >= t, scores, 0.0)
            total = total + dot(scores.astype(BF), v)
            total = total + nt(lifted.astype(BF), start[d, n])
            lifted_o[d, rows] = (lifted * jnp.exp(passed[d, n : n + 1])).astype(BF)
        local_o[rows] = total


def readout_kernel(place, local, lifted, every, before, rescale, gate, out):
    z = place[0]
    summed = local[...]
    for d in range(2):
        state = jnp.zeros((HEAD, HEAD), F32)
        for k in range(8) if d == 0 else reversed(range(8)):
            new, step = unpack(every[k])
            state = jnp.where(k < z if d == 0 else k > z, jnp.exp(step) * state + new, state)
        incoming = before[d, :HEAD] + jnp.exp(before[d, HEAD : HEAD + 1]) * state
        summed = summed + nt(lifted[d], incoming.astype(BF))
    factor = lax.rsqrt(jnp.mean(summed * summed, axis=-1, keepdims=True) + 1e-06)
    out[...] = (summed * factor * rescale[...].astype(F32) * gate[...]).astype(BF)


def project_out_kernel(place, rec, conv, columns, out):
    core = place[0]
    at = [pl.multiple_of(k * 96 + core * 48, 16) for k in range(4)]
    left = jnp.concatenate([rec[pl.ds(k, 48)] for k in at], axis=0)
    right = jnp.concatenate([conv[pl.ds(k, 48)] for k in at], axis=0)
    rows = jnp.concatenate([left, right], axis=1)
    for c in range(0, 2048, 512):
        part = nt(rows, columns[c : c + 512])
        for k in range(4):
            out[k, :, c : c + 512] = part[k * 48 : (k + 1) * 48].astype(out.dtype)


def meet_kernel(place, mine, got, far_low, far_high, ahead, behind, own):
    y = place[3]

    def block(step):
        k = lax.rem(y + step, 4)
        return mine[k] + got[k].astype(F32)

    far = block(2)
    far_low[...] = far[:, :1024].astype(BF)
    far_high[...] = far[:, 1024:].astype(BF)
    ahead[...] = block(1)
    behind[...] = block(3)
    own[...] = block(0)


def relay_kernel(ahead, behind, low, high, ahead_o, behind_o):
    ahead_o[:, :1024] = (ahead[:, :1024] + low[...].astype(F32)).astype(BF)
    ahead_o[:, 1024:] = ahead[:, 1024:].astype(BF)
    behind_o[:, :1024] = behind[:, :1024].astype(BF)
    behind_o[:, 1024:] = (behind[:, 1024:] + high[...].astype(F32)).astype(BF)


def on_device(
    sequence_embeddings,
    entry_rescale_vector,
    probe_matrix,
    onward_retain_matrix,
    reverse_retain_matrix,
    content_matrix,
    emission_switch_matrix,
    pointwise_content_matrix,
    pointwise_switch_matrix,
    retain_lower_slack,
    extra_log_shrink,
    subspace_rescale,
    filter_kernel_coefs,
    channel_cluster_scale,
    scan_readout_matrix,
    filter_readout_matrix,
):
    x, z, y = (lax.axis_index(axis) for axis in "xzy")
    core = lax.axis_index("core")
    length = sequence_embeddings.shape[0]
    gain = entry_rescale_vector[None]
    place = jnp.stack([z, lax.rem(4 - x, 4) * 64, x, y]).astype(jnp.int32)
    first, shard = kernel_call(
        collect_kernel,
        "collect",
        2,
        [pltpu.VMEM((8, 64, 384), BF), pltpu.VMEM((64, 768), BF)],
        *(
            far_off(weight)
            for weight in (
                onward_retain_matrix,
                reverse_retain_matrix,
                content_matrix,
                probe_matrix,
                emission_switch_matrix,
                pointwise_content_matrix,
                pointwise_switch_matrix,
                scan_readout_matrix.T,
                filter_readout_matrix.T,
            )
        ),
    )
    first = lax.all_to_all(first, "z", 0, 0, tiled=True).reshape(512, 384)
    ahead, far, behind = shift(shard, "x", -1), shift(shard, "x", 2), shift(shard, "x", 1)
    normed, normed_first = normalized(place, far_off(sequence_embeddings), gain, 2)
    normed, normed_first, shard, ahead, far, behind, first = lax.optimization_barrier(
        (normed, normed_first, shard, ahead, far, behind, first)
    )
    (later,) = kernel_call(
        stack_kernel,
        "stack",
        1,
        [pltpu.HBM((256, 768), BF)],
        keep(shard),
        keep(ahead),
        keep(far),
        keep(behind),
    )
    weights = lax.all_gather(later, "z", axis=0, tiled=True)
    ahead, behind = shift(first, "x", -1), shift(first, "x", 1)
    far_low, far_high = shift(behind[:256], "x", 1), shift(ahead[256:], "x", -1)
    edges = jnp.concatenate(
        [
            line(sequence_embeddings[-16:], ("z", "x"), 1),
            line(sequence_embeddings[:16], ("z", "x"), -1),
        ],
        axis=0,
    )
    far_low, far_high, edges = lax.optimization_barrier((far_low, far_high, edges))
    (edges,) = normalized(place, edges, gain, 1)
    normed_first = keep(normed_first)
    (near,) = kernel_call(
        near_scores_kernel,
        "near",
        2,
        [pltpu.VMEM((length, 384), F32)],
        normed_first,
        keep(first),
        keep(ahead),
        keep(behind),
    )
    blocks = length // BLOCK
    values, gap, cum, start, passed, send = kernel_call(
        gates_kernel,
        "gates",
        3,
        [
            pltpu.HBM((length, HEAD), BF),
            pltpu.HBM((2, length, HEAD), F32),
            pltpu.HBM((2, length, HEAD), F32),
            pltpu.HBM((2, blocks, HEAD, HEAD), BF),
            pltpu.HBM((2, 8, HEAD), F32),
            pltpu.VMEM((4, 2, PACK, HEAD), BF),
        ],
        keep(near),
        normed_first,
        keep(far_low),
        keep(far_high),
        retain_lower_slack,
        extra_log_shrink,
    )
    got = lax.all_to_all(send, "x", 0, 0, tiled=True)
    before, send = kernel_call(
        row_kernel,
        "row",
        1,
        [pltpu.HBM((2, HEAD + 8, HEAD), F32), pltpu.VMEM((8, PACK, HEAD), BF)],
        place,
        keep(got),
    )
    every = lax.all_to_all(send, "z", 0, 0, tiled=True)

    local, lifted, gate, conv_out, columns = kernel_call(
        later_kernel,
        "later",
        6,
        [
            pltpu.HBM((length, HEAD), F32),
            pltpu.HBM((2, length, HEAD), BF),
            pltpu.HBM((length, HEAD), F32),
            pltpu.VMEM((length, HEAD), BF),
            pltpu.VMEM((2048, 256), BF),
        ],
        place,
        keep(normed),
        keep(edges),
        *(far_off(a) for a in (weights, values, gap, cum, start, passed)),
        filter_kernel_coefs,
        channel_cluster_scale[None],
        scratch=(pltpu.VMEM((length, HEAD), F32), pltpu.VMEM((length + 32, HEAD), F32)),
    )
    (rec_out,) = kernel_call(
        readout_kernel,
        "readout",
        1,
        [pltpu.VMEM((length, HEAD), BF)],
        place,
        far_off(local),
        far_off(lifted),
        keep(every),
        far_off(before),
        subspace_rescale[None],
        far_off(gate),
    )
    theirs, mine = (
        kernel_call(
            project_out_kernel,
            "project_out",
            1,
            [pltpu.VMEM((4, 48, 2048), kind)],
            side[None].astype(jnp.int32),
            keep(rec_out),
            keep(conv_out),
            keep(columns),
        )[0]
        for side, kind in ((1 - core, BF), (core, F32))
    )
    half, whole, final = (
        pltpu.VMEM((48, 1024), BF),
        pltpu.VMEM((48, 2048), F32),
        pltpu.VMEM((48, 2048), BF),
    )
    far_low, far_high, ahead, behind, own = kernel_call(
        meet_kernel,
        "meet",
        1,
        [half, half, whole, whole, whole],
        place,
        keep(mine),
        keep(shift(theirs, "core", 1)),
    )
    ahead, behind = kernel_call(
        relay_kernel,
        "relay",
        0.5,
        [final, final],
        keep(ahead),
        keep(behind),
        keep(shift(far_low, "y", 1)),
        keep(shift(far_high, "y", -1)),
    )
    ahead, behind = shift(ahead, "y", 1), shift(behind, "y", -1)
    return (own + ahead.astype(F32) + behind.astype(F32)).astype(BF)


def solution(mesh):
    finer = Mesh(mesh.devices.reshape(8, 4, 4, 2), ("z", "x", "y", "core"))
    sp, tp = ("z", "x"), ("y", "core")
    in_specs = (
        P(sp, None),
        P(),
        *(P(sp, tp) for _ in range(7)),
        P(None, tp),
        P(None, sp, tp),
        P(),
        P(None, tp),
        P(tp),
        P(tp, sp),
        P(tp, sp),
    )
    return jax.shard_map(
        on_device,
        mesh=finer,
        in_specs=in_specs,
        out_specs=P((*sp, *tp), None),
        check_vma=False,
    )
```

```python
import jax
import jax.numpy as jnp
from jax import lax
from jax.experimental import pallas as pl
from jax.experimental.pallas import tpu as pltpu
from jax.sharding import Mesh
from jax.sharding import PartitionSpec as P


CONV_KW = 31
BLOCK = 64
HEAD = 128
PACK = 144
BF = jnp.bfloat16
F32 = jnp.float32
ROOM = pltpu.CompilerParams(vmem_limit_bytes=24 * 2**20)
SMEM = pl.BlockSpec(memory_space=pltpu.SMEM)
VMEM = pl.BlockSpec(memory_space=pltpu.VMEM)
ANY = pl.BlockSpec(memory_space=pl.ANY)


def ring(count, step):
    return [(i, (i + step) % count) for i in range(count)]


def shift(array, axis, step):
    return lax.ppermute(array, axis, ring(lax.axis_size(axis), step))


def line(array, axes, step):
    count = lax.axis_size(axes)
    pairs = [(i, i + step) for i in range(count) if 0 <= i + step < count]
    return lax.ppermute(array, axes, pairs)


def ordered(first, *arrays):
    return lax.optimization_barrier((first, *arrays))


def keep(array):
    return pltpu.with_memory_space_constraint(array, pltpu.VMEM)


def far_off(array):
    return pltpu.with_memory_space_constraint(array, pltpu.HBM)


def kernel_call(body, micros, outs, *operands, scratch=(), left=()):
    return pl.pallas_call(
        body,
        out_shape=tuple(outs),
        in_specs=[
            SMEM if o.dtype == jnp.int32 else ANY if k in left else VMEM
            for k, o in enumerate(operands)
        ],
        scratch_shapes=list(scratch),
        compiler_params=ROOM,
        cost_estimate=pl.CostEstimate(
            flops=int(micros * 4e6), transcendentals=0, bytes_accessed=0
        ),
    )(*operands)


def nt(a, b):
    return lax.dot_general(a, b, (((1,), (1,)), ((), ())), preferred_element_type=F32)


def tn(a, b):
    return lax.dot_general(a, b, (((0,), (0,)), ((), ())), preferred_element_type=F32)


def dot(a, b):
    return jnp.dot(a, b, preferred_element_type=F32)


def collect_kernel(x, *refs):
    first, later, top, bottom, done = refs[-5:]
    edge = top.shape[0]
    rows = (x.at[:edge], x.at[x.shape[0] - edge :])
    copies = [
        pltpu.make_async_copy(source, into, done.at[k])
        for k, (source, into) in enumerate(zip(rows, (top, bottom)))
    ]
    for copy in copies:
        copy.start()
    for k, ref in enumerate(refs[:3]):
        for z in range(8):
            first[z, :, k * HEAD : (k + 1) * HEAD] = ref[...]
    for k, ref in enumerate(refs[3:-5]):
        later[:, k * HEAD : (k + 1) * HEAD] = ref[...]
    for copy in copies:
        copy.wait()


def stack_kernel(own, ahead, far, behind, later):
    for k, ref in enumerate((own, ahead, far, behind)):
        later[k * 64 : (k + 1) * 64] = ref[...]


def normalize_kernel(place, x, gain, out, *other):
    turn = place[1]
    floats = x[...].astype(F32)
    factor = lax.rsqrt(jnp.mean(floats * floats, axis=-1, keepdims=True) + 1e-06)
    low = lax.broadcasted_iota(jnp.int32, (x.shape[0], HEAD), 1) < 64
    for pair in range(4):
        pieces = []
        for k in (2 * pair, 2 * pair + 1):
            at = slice(k * 256, (k + 1) * 256)
            scaled = x[:, at].astype(F32) * factor * gain[:, at].astype(F32)
            turned = pltpu.roll(scaled, turn, 1)
            out[:, at] = turned.astype(BF)
            pieces.append((turned[:, :HEAD], turned[:, HEAD:]))
        if other:
            for half in range(2):
                one, two = pieces[0][half], pieces[1][half]
                even = jnp.where(low, one, pltpu.roll(two, 64, 1))
                odd = jnp.where(low, pltpu.roll(one, 64, 1), two)
                for piece, value in ((2 * half, even), (2 * half + 1, odd)):
                    at = piece * 512 + pair * HEAD
                    other[0][:, at : at + HEAD] = value.astype(BF)


def normalized(place, x, gain, count):
    outs = [pltpu.VMEM(x.shape, BF)] * count
    return kernel_call(normalize_kernel, 3, outs, place, x, gain)


def near_scores_kernel(normed, own, ahead, behind, out):
    total = dot(normed[:, :512], own[...])
    total = total + dot(normed[:, 512:1024], ahead[...])
    out[...] = total + dot(normed[:, 1536:], behind[...])


def pack(state, log):
    high = log.astype(BF).astype(F32)
    pad = jnp.zeros((PACK - HEAD - 8, HEAD), F32)
    rows = lax.broadcasted_iota(jnp.int32, (8, HEAD), 0)
    logs = jnp.where(rows == 0, high, jnp.where(rows == 1, log - high, 0.0))
    return jnp.concatenate([state, logs, pad], axis=0).astype(BF)


def unpack(message):
    state = message[:HEAD].astype(F32)
    logs = message[HEAD:PACK].astype(F32)
    return state, logs[0:1] + logs[1:2]


def gates_kernel(near, normed, far_low, far_high, slack, extra, values_o, gap_o, cum_o, start_o, passed_o, send):
    length = near.shape[0]
    blocks = length // BLOCK
    scores = near[...] + dot(normed[:, 1024:1280], far_low[...])
    scores = scores + dot(normed[:, 1280:1536], far_high[...])
    inside = lax.rem(lax.broadcasted_iota(jnp.int32, (length, HEAD), 0), BLOCK)
    v = scores[:, 256:].astype(BF)
    values_o[...] = v
    for d in range(2):
        gap = slack[d : d + 1, :] * jax.nn.sigmoid(-scores[:, d * HEAD : (d + 1) * HEAD])
        cum = jnp.log1p(-gap) + extra[d]
        step = 1
        while step < BLOCK:
            if d == 0:
                moved = jnp.where(inside >= step, pltpu.roll(cum, step, 0), 0.0)
            else:
                moved = jnp.where(inside < BLOCK - step, pltpu.roll(cum, length - step, 0), 0.0)
            cum = cum + moved
            step *= 2
        gap_o[d] = gap
        cum_o[d] = cum
        state = jnp.zeros((HEAD, HEAD), F32)
        passed = jnp.zeros((1, HEAD), F32)
        for n in range(blocks) if d == 0 else reversed(range(blocks)):
            rows = slice(n * BLOCK, (n + 1) * BLOCK)
            last = n * BLOCK + (BLOCK - 1 if d == 0 else 0)
            total = cum[last : last + 1]
            fade = gap[rows] * jnp.exp(total - cum[rows])
            start_o[d, n] = state.astype(BF)
            passed_o[d, n : n + 1] = passed
            state = jnp.exp(total) * state + tn(v[rows], fade.astype(BF))
            passed = passed + total
        send[d] = pack(state, passed)


def row_kernel(place, own, ahead, far, behind, before_o, send, got):
    x, z = place[2], place[0]
    for k, ref in enumerate((own, ahead, far, behind)):
        got[lax.rem(x + k, 4)] = ref[...]
    messages = []
    for d in range(2):
        state = jnp.zeros((HEAD, HEAD), F32)
        log = jnp.zeros((1, HEAD), F32)
        before, passed = state, log
        for k in range(4) if d == 0 else reversed(range(4)):
            before = jnp.where(k == x, state, before)
            passed = jnp.where(k == x, log, passed)
            new, step = unpack(got[k, d])
            state = jnp.exp(step) * state + new
            log = log + step
        before_o[d, :HEAD] = before
        before_o[d, HEAD : HEAD + 8] = jnp.broadcast_to(passed, (8, HEAD))
        messages.append(pack(state, log))
    for k in range(8):
        send[k] = jnp.where(k > z, messages[0], messages[1])


def later_kernel(place, normed, edges, *refs):
    pieces = refs[:9]
    values, gap, cum, start, passed, taps, scale = refs[9:16]
    local_o, lifted_o, gate_o, conv_o, columns_o, query, glu, weights, done = refs[16:]
    x, z_here = place[2], place[0]
    copies = []
    for k, piece in enumerate(pieces):
        step, inside = (k, 0) if k < 5 else (k - 1, 128 if k == 5 else 0)
        to = pl.multiple_of(lax.rem(z_here + step, 8) * 256 + inside, 128)
        into = weights.at[pl.ds(to, piece.shape[0])]
        copies.append(pltpu.make_async_copy(piece, into, done.at[k]))
        copies[-1].start()
    for copy in copies:
        copy.wait()
    length = normed.shape[0]
    blocks = length // BLOCK
    pre = dot(normed[...], weights[:, :256])
    query[...] = pre[:, :HEAD] * jax.nn.sigmoid(pre[:, :HEAD])
    gate_o[...] = pre[:, HEAD:] * jax.nn.sigmoid(pre[:, HEAD:])

    def gated(rows):
        pair = dot(rows, weights[:, 256:512])
        return (pair[:, :HEAD] * jax.nn.sigmoid(pair[:, HEAD:])).astype(BF).astype(F32)

    glu[16 : 16 + length] = gated(normed[...])
    edge = gated(edges[...])
    glu[:16] = edge[:16]
    glu[16 + length :] = edge[16:]
    framed = glu[...]
    kernel = taps[...].astype(F32)
    total = None
    for r in range(8):
        turned = framed if r == 0 else pltpu.roll(framed, length + 32 - r, 0)
        for j in range(CONV_KW):
            if (1 + j) % 8 == r:
                at = (1 + j) - r
                part = turned[at : at + length] * kernel[j : j + 1]
                total = part if total is None else total + part
    centred = total - jnp.mean(total, axis=-1, keepdims=True)
    variance = jnp.mean(centred * centred, axis=-1, keepdims=True)
    standard = centred * lax.rsqrt(variance + 1e-05) * scale[...].astype(F32)
    conv_o[...] = (standard * jax.nn.sigmoid(standard)).astype(BF)

    for k in range(4):
        turn = lax.rem(x + k, 4)
        for z in range(8):
            to = pl.multiple_of((z * 4 + turn) * 64, 64)
            at = (z * 4 + k) * 64
            columns_o[pl.ds(to, 64)] = weights[at : at + 64, 512:768]

    t = lax.broadcasted_iota(jnp.int32, (BLOCK, BLOCK), 0)
    s = lax.broadcasted_iota(jnp.int32, (BLOCK, BLOCK), 1)
    for n in range(blocks):
        rows = slice(n * BLOCK, (n + 1) * BLOCK)
        q = query[rows]
        v = values[rows]
        total = jnp.zeros((BLOCK, HEAD), F32)
        for d in range(2):
            c = cum[d, rows]
            lifted = q * jnp.exp(c)
            lowered = gap[d, rows] * jnp.exp(-c)
            scores = nt(lifted.astype(BF), lowered.astype(BF))
            scores = jnp.where(s <= t if d == 0 else s >= t, scores, 0.0)
            total = total + dot(scores.astype(BF), v)
            total = total + nt(lifted.astype(BF), start[d, n])
            lifted_o[d, rows] = (lifted * jnp.exp(passed[d, n : n + 1])).astype(BF)
        local_o[rows] = total


def readout_kernel(place, local, lifted, every, before, rescale, gate, out):
    z = place[0]
    summed = local[...]
    for d in range(2):
        state = jnp.zeros((HEAD, HEAD), F32)
        for k in range(8) if d == 0 else reversed(range(8)):
            new, step = unpack(every[k])
            state = jnp.where(k < z if d == 0 else k > z, jnp.exp(step) * state + new, state)
        incoming = before[d, :HEAD] + jnp.exp(before[d, HEAD : HEAD + 1]) * state
        summed = summed + nt(lifted[d], incoming.astype(BF))
    factor = lax.rsqrt(jnp.mean(summed * summed, axis=-1, keepdims=True) + 1e-06)
    out[...] = (summed * factor * rescale[...].astype(F32) * gate[...]).astype(BF)


def project_out_kernel(place, rec, conv, columns, out):
    core = place[0]
    at = [pl.multiple_of(k * 96 + core * 48, 16) for k in range(4)]
    left = jnp.concatenate([rec[pl.ds(k, 48)] for k in at], axis=0)
    right = jnp.concatenate([conv[pl.ds(k, 48)] for k in at], axis=0)
    rows = jnp.concatenate([left, right], axis=1)
    for c in range(0, 2048, 512):
        part = nt(rows, columns[c : c + 512])
        for k in range(4):
            out[k, :, c : c + 512] = part[k * 48 : (k + 1) * 48].astype(out.dtype)


def meet_kernel(place, mine, got, far_low, far_high, ahead, behind, own):
    y = place[3]

    def block(step):
        k = lax.rem(y + step, 4)
        return mine[k] + got[k].astype(F32)

    far = block(2)
    far_low[...] = far[:, :1024].astype(BF)
    far_high[...] = far[:, 1024:].astype(BF)
    ahead[...] = block(1)
    behind[...] = block(3)
    own[...] = block(0)


def relay_kernel(ahead, behind, low, high, ahead_o, behind_o):
    ahead_o[:, :1024] = (ahead[:, :1024] + low[...].astype(F32)).astype(BF)
    ahead_o[:, 1024:] = ahead[:, 1024:].astype(BF)
    behind_o[:, :1024] = behind[:, :1024].astype(BF)
    behind_o[:, 1024:] = (behind[:, 1024:] + high[...].astype(F32)).astype(BF)


def layer(
    sequence_embeddings,
    entry_rescale_vector,
    probe_matrix,
    onward_retain_matrix,
    reverse_retain_matrix,
    content_matrix,
    emission_switch_matrix,
    pointwise_content_matrix,
    pointwise_switch_matrix,
    retain_lower_slack,
    extra_log_shrink,
    subspace_rescale,
    filter_kernel_coefs,
    channel_cluster_scale,
    scan_readout_matrix,
    filter_readout_matrix,
):
    x, z, y = (lax.axis_index(axis) for axis in "xzy")
    core = lax.axis_index("core")
    length = sequence_embeddings.shape[0]
    gain = entry_rescale_vector[None]
    place = jnp.stack([z, lax.rem(4 - x, 4) * 64, x, y]).astype(jnp.int32)
    edge = pltpu.VMEM((16, sequence_embeddings.shape[1]), BF)
    first, shard, top, bottom = kernel_call(
        collect_kernel,
        2,
        [pltpu.VMEM((8, 64, 384), BF), pltpu.VMEM((64, 768), BF), edge, edge],
        far_off(sequence_embeddings),
        *(
            far_off(weight)
            for weight in (
                onward_retain_matrix,
                reverse_retain_matrix,
                content_matrix,
                probe_matrix,
                emission_switch_matrix,
                pointwise_content_matrix,
                pointwise_switch_matrix,
                scan_readout_matrix.T,
                filter_readout_matrix.T,
            )
        ),
        scratch=(pltpu.SemaphoreType.DMA((2,)),),
        left=(0,),
    )
    first = lax.all_to_all(first, "z", 0, 0, tiled=True).reshape(512, 384)
    ahead, far, behind = shift(shard, "x", -1), shift(shard, "x", 2), shift(shard, "x", 1)
    normed, normed_first = normalized(place, far_off(sequence_embeddings), gain, 2)
    low, high = line(bottom, ("z", "x"), 1), line(top, ("z", "x"), -1)
    normed, normed_first, shard, ahead, far, behind, low, high = lax.optimization_barrier(
        (normed, normed_first, shard, ahead, far, behind, low, high)
    )
    (edges,) = normalized(place, jnp.concatenate([low, high], axis=0), gain, 1)
    (later,) = kernel_call(
        stack_kernel,
        1,
        [pltpu.HBM((256, 768), BF)],
        keep(shard),
        keep(ahead),
        keep(far),
        keep(behind),
    )
    _, later = ordered(first, later)
    ahead, behind = shift(first, "x", -1), shift(first, "x", 1)
    up1, down1 = shift(later, "z", 1), shift(later, "z", -1)
    far_low, far_high = shift(behind[:256], "x", 1), shift(ahead[256:], "x", -1)
    normed_first = keep(normed_first)
    (near,) = kernel_call(
        near_scores_kernel,
        2,
        [pltpu.VMEM((length, 384), F32)],
        normed_first,
        keep(first),
        keep(ahead),
        keep(behind),
    )
    _, up1, down1 = ordered(near, up1, down1)
    up2, down2 = shift(up1, "z", 1), shift(down1, "z", -1)
    blocks = length // BLOCK
    values, gap, cum, start, passed, send = kernel_call(
        gates_kernel,
        3,
        [
            pltpu.HBM((length, HEAD), BF),
            pltpu.HBM((2, length, HEAD), F32),
            pltpu.HBM((2, length, HEAD), F32),
            pltpu.HBM((2, blocks, HEAD, HEAD), BF),
            pltpu.HBM((2, 8, HEAD), F32),
            pltpu.VMEM((2, PACK, HEAD), BF),
        ],
        keep(near),
        normed_first,
        keep(far_low),
        keep(far_high),
        retain_lower_slack,
        extra_log_shrink,
    )
    row = [send, shift(send, "x", -1), shift(send, "x", 2), shift(send, "x", 1)]
    _, up2, down2 = ordered(send, up2, down2)
    up3, down3 = shift(up2, "z", 1), shift(down2, "z", -1)
    before, send = kernel_call(
        row_kernel,
        1,
        [pltpu.HBM((2, HEAD + 8, HEAD), F32), pltpu.VMEM((8, PACK, HEAD), BF)],
        place,
        *(keep(piece) for piece in row),
        scratch=(pltpu.VMEM((4, 2, PACK, HEAD), BF),),
    )
    _, up3, down3 = ordered(send, up3, down3)
    low4, high4 = shift(up3[:128], "z", 1), shift(down3[128:], "z", -1)
    every = lax.all_to_all(send, "z", 0, 0, tiled=True)

    local, lifted, gate, conv_out, columns = kernel_call(
        later_kernel,
        0.5,
        [
            pltpu.HBM((length, HEAD), F32),
            pltpu.HBM((2, length, HEAD), BF),
            pltpu.HBM((length, HEAD), F32),
            pltpu.VMEM((length, HEAD), BF),
            pltpu.VMEM((2048, 256), BF),
        ],
        place,
        keep(normed),
        keep(edges),
        *(far_off(a) for a in (later, down1, down2, down3, low4, high4, up3, up2, up1)),
        *(far_off(a) for a in (values, gap, cum, start, passed)),
        filter_kernel_coefs,
        channel_cluster_scale[None],
        scratch=(
            pltpu.VMEM((length, HEAD), F32),
            pltpu.VMEM((length + 32, HEAD), F32),
            pltpu.VMEM((2048, 768), BF),
            pltpu.SemaphoreType.DMA((9,)),
        ),
        left=range(3, 12),
    )
    (rec_out,) = kernel_call(
        readout_kernel,
        1,
        [pltpu.VMEM((length, HEAD), BF)],
        place,
        far_off(local),
        far_off(lifted),
        keep(every),
        far_off(before),
        subspace_rescale[None],
        far_off(gate),
    )
    theirs, mine = (
        kernel_call(
            project_out_kernel,
            1,
            [pltpu.VMEM((4, 48, 2048), kind)],
            side[None].astype(jnp.int32),
            keep(rec_out),
            keep(conv_out),
            keep(columns),
        )[0]
        for side, kind in ((1 - core, BF), (core, F32))
    )
    half, whole, final = (
        pltpu.VMEM((48, 1024), BF),
        pltpu.VMEM((48, 2048), F32),
        pltpu.VMEM((48, 2048), BF),
    )
    far_low, far_high, ahead, behind, own = kernel_call(
        meet_kernel,
        1,
        [half, half, whole, whole, whole],
        place,
        keep(mine),
        keep(shift(theirs, "core", 1)),
    )
    ahead, behind = kernel_call(
        relay_kernel,
        0.5,
        [final, final],
        keep(ahead),
        keep(behind),
        keep(shift(far_low, "y", 1)),
        keep(shift(far_high, "y", -1)),
    )
    ahead, behind = shift(ahead, "y", 1), shift(behind, "y", -1)
    return (own + ahead.astype(F32) + behind.astype(F32)).astype(BF)


def solution(mesh):
    finer = Mesh(mesh.devices.reshape(8, 4, 4, 2), ("z", "x", "y", "core"))
    sp, tp = ("z", "x"), ("y", "core")
    in_specs = (
        P(sp, None),
        P(),
        *(P(sp, tp) for _ in range(7)),
        P(None, tp),
        P(None, sp, tp),
        P(),
        P(None, tp),
        P(tp),
        P(tp, sp),
        P(tp, sp),
    )
    return jax.shard_map(
        layer,
        mesh=finer,
        in_specs=in_specs,
        out_specs=P((*sp, *tp), None),
        check_vma=False,
    )
```

```python
import jax
import jax.numpy as jnp
from jax import lax
from jax.experimental import pallas as pl
from jax.experimental.pallas import tpu as pltpu
from jax.sharding import Mesh
from jax.sharding import PartitionSpec as P


CONV_KW = 31
BLOCK = 64
HEAD = 128
PACK = 144
BF = jnp.bfloat16
F32 = jnp.float32
ROOM = pltpu.CompilerParams(vmem_limit_bytes=24 * 2**20)
SMEM = pl.BlockSpec(memory_space=pltpu.SMEM)
VMEM = pl.BlockSpec(memory_space=pltpu.VMEM)
ANY = pl.BlockSpec(memory_space=pl.ANY)


def ring(count, step):
    return [(i, (i + step) % count) for i in range(count)]


def shift(array, axis, step):
    return lax.ppermute(array, axis, ring(lax.axis_size(axis), step))


def line(array, axes, step):
    count = lax.axis_size(axes)
    pairs = [(i, i + step) for i in range(count) if 0 <= i + step < count]
    return lax.ppermute(array, axes, pairs)


def ordered(first, *arrays):
    return lax.optimization_barrier((first, *arrays))


def keep(array):
    return pltpu.with_memory_space_constraint(array, pltpu.VMEM)


def far_off(array):
    return pltpu.with_memory_space_constraint(array, pltpu.HBM)


def kernel_call(body, micros, outs, *operands, scratch=(), left=()):
    return pl.pallas_call(
        body,
        out_shape=tuple(outs),
        in_specs=[
            SMEM if o.dtype == jnp.int32 else ANY if k in left else VMEM
            for k, o in enumerate(operands)
        ],
        scratch_shapes=list(scratch),
        compiler_params=ROOM,
        cost_estimate=pl.CostEstimate(
            flops=int(micros * 4e6), transcendentals=0, bytes_accessed=0
        ),
    )(*operands)


def nt(a, b):
    return lax.dot_general(a, b, (((1,), (1,)), ((), ())), preferred_element_type=F32)


def tn(a, b):
    return lax.dot_general(a, b, (((0,), (0,)), ((), ())), preferred_element_type=F32)


def dot(a, b):
    return jnp.dot(a, b, preferred_element_type=F32)


def collect_kernel(x, *refs):
    first, later, top, bottom, done = refs[-5:]
    edge = top.shape[0]
    rows = (x.at[:edge], x.at[x.shape[0] - edge :])
    copies = [
        pltpu.make_async_copy(source, into, done.at[k])
        for k, (source, into) in enumerate(zip(rows, (top, bottom)))
    ]
    for copy in copies:
        copy.start()
    for k, ref in enumerate(refs[:3]):
        for z in range(8):
            first[z, :, k * HEAD : (k + 1) * HEAD] = ref[...]
    for k, ref in enumerate(refs[3:-5]):
        later[:, k * HEAD : (k + 1) * HEAD] = ref[...]
    for copy in copies:
        copy.wait()


def stack_kernel(own, ahead, far, behind, later):
    for k, ref in enumerate((own, ahead, far, behind)):
        later[k * 64 : (k + 1) * 64] = ref[...]


def normalize_kernel(place, x, gain, out, *other):
    turn = place[1]
    floats = x[...].astype(F32)
    factor = lax.rsqrt(jnp.mean(floats * floats, axis=-1, keepdims=True) + 1e-06)
    low = lax.broadcasted_iota(jnp.int32, (x.shape[0], HEAD), 1) < 64
    for pair in range(4):
        pieces = []
        for k in (2 * pair, 2 * pair + 1):
            at = slice(k * 256, (k + 1) * 256)
            scaled = x[:, at].astype(F32) * factor * gain[:, at].astype(F32)
            turned = pltpu.roll(scaled, turn, 1)
            out[:, at] = turned.astype(BF)
            pieces.append((turned[:, :HEAD], turned[:, HEAD:]))
        if other:
            for half in range(2):
                one, two = pieces[0][half], pieces[1][half]
                even = jnp.where(low, one, pltpu.roll(two, 64, 1))
                odd = jnp.where(low, pltpu.roll(one, 64, 1), two)
                for piece, value in ((2 * half, even), (2 * half + 1, odd)):
                    at = piece * 512 + pair * HEAD
                    other[0][:, at : at + HEAD] = value.astype(BF)


def normalized(place, x, gain, count):
    outs = [pltpu.VMEM(x.shape, BF), pltpu.VMEM(x.shape, BF)][:count]
    if count == 2:
        outs[0] = pltpu.HBM(x.shape, BF)
    return kernel_call(normalize_kernel, 3, outs, place, x, gain)


def near_scores_kernel(normed, own, ahead, behind, out):
    total = dot(normed[:, :512], own[...])
    total = total + dot(normed[:, 512:1024], ahead[...])
    out[...] = total + dot(normed[:, 1536:], behind[...])


def pack(state, log):
    high = log.astype(BF).astype(F32)
    pad = jnp.zeros((PACK - HEAD - 8, HEAD), F32)
    rows = lax.broadcasted_iota(jnp.int32, (8, HEAD), 0)
    logs = jnp.where(rows == 0, high, jnp.where(rows == 1, log - high, 0.0))
    return jnp.concatenate([state, logs, pad], axis=0).astype(BF)


def unpack(message):
    state = message[:HEAD].astype(F32)
    logs = message[HEAD:PACK].astype(F32)
    return state, logs[0:1] + logs[1:2]


def gates_kernel(near, normed, far_low, far_high, slack, extra, values_o, gap_o, cum_o, start_o, passed_o, send):
    length = near.shape[0]
    blocks = length // BLOCK
    scores = near[...] + dot(normed[:, 1024:1280], far_low[...])
    scores = scores + dot(normed[:, 1280:1536], far_high[...])
    inside = lax.rem(lax.broadcasted_iota(jnp.int32, (length, HEAD), 0), BLOCK)
    v = scores[:, 256:].astype(BF)
    values_o[...] = v
    for d in range(2):
        gap = slack[d : d + 1, :] * jax.nn.sigmoid(-scores[:, d * HEAD : (d + 1) * HEAD])
        cum = jnp.log1p(-gap) + extra[d]
        step = 1
        while step < BLOCK:
            if d == 0:
                moved = jnp.where(inside >= step, pltpu.roll(cum, step, 0), 0.0)
            else:
                moved = jnp.where(inside < BLOCK - step, pltpu.roll(cum, length - step, 0), 0.0)
            cum = cum + moved
            step *= 2
        gap_o[d] = gap
        cum_o[d] = cum
        state = jnp.zeros((HEAD, HEAD), F32)
        passed = jnp.zeros((1, HEAD), F32)
        for n in range(blocks) if d == 0 else reversed(range(blocks)):
            rows = slice(n * BLOCK, (n + 1) * BLOCK)
            last = n * BLOCK + (BLOCK - 1 if d == 0 else 0)
            total = cum[last : last + 1]
            fade = gap[rows] * jnp.exp(total - cum[rows])
            start_o[d, n] = state.astype(BF)
            passed_o[d, n : n + 1] = passed
            state = jnp.exp(total) * state + tn(v[rows], fade.astype(BF))
            passed = passed + total
        send[d] = pack(state, passed)


def row_kernel(place, own, ahead, far, behind, before_o, send, got):
    x, z = place[2], place[0]
    for k, ref in enumerate((own, ahead, far, behind)):
        got[lax.rem(x + k, 4)] = ref[...]
    messages = []
    for d in range(2):
        state = jnp.zeros((HEAD, HEAD), F32)
        log = jnp.zeros((1, HEAD), F32)
        before, passed = state, log
        for k in range(4) if d == 0 else reversed(range(4)):
            before = jnp.where(k == x, state, before)
            passed = jnp.where(k == x, log, passed)
            new, step = unpack(got[k, d])
            state = jnp.exp(step) * state + new
            log = log + step
        before_o[d, :HEAD] = before
        before_o[d, HEAD : HEAD + 8] = jnp.broadcast_to(passed, (8, HEAD))
        messages.append(pack(state, log))
    for k in range(8):
        send[k] = jnp.where(k > z, messages[0], messages[1])


def spread(place, pieces, steps):
    z = place[0]
    found = []
    for piece, (step, inside) in zip(pieces, steps):
        at = pl.multiple_of(lax.rem(z + step, 8) * 256 + inside, 128)
        found.append((piece, at, piece.shape[0]))
    return found


NEAR_STEPS = ((0, 0), (1, 0), (2, 0), (6, 0), (7, 0))
FAR_STEPS = ((3, 0), (4, 0), (4, 128), (5, 0))


def early_kernel(place, normed, edges, *refs):
    pieces = refs[:5]
    gap, cum = refs[5:7]
    scores_o, edge_o, lowered_o, grown_o, held, done = refs[7:]
    copies = []
    for k, piece in enumerate(pieces):
        copies.append(pltpu.make_async_copy(piece.at[:, :512], held.at[k], done.at[k]))
        copies[-1].start()
    for d in range(2):
        grown = jnp.exp(cum[d])
        grown_o[d] = grown
        lowered_o[d] = (gap[d] * jnp.exp(-cum[d])).astype(BF)
    for copy in copies:
        copy.wait()
    total, edge = None, None
    for k, (piece, at, count) in enumerate(spread(place, pieces, NEAR_STEPS)):
        part = dot(normed[:, pl.ds(at, count)], held[k])
        total = part if total is None else total + part
        part = dot(edges[:, pl.ds(at, count)], held[k, :, 256:])
        edge = part if edge is None else edge + part
    scores_o[...] = total
    edge_o[...] = edge


def later_kernel(place, normed, edges, scores, edge_scores, *refs):
    near, far = refs[:5], refs[5:9]
    values, lowered, grown, start, passed, taps, scale = refs[9:16]
    local_o, lifted_o, gate_o, conv_o, columns_o, query, glu, held, done, placed = refs[16:]
    x = place[2]
    length = normed.shape[0]
    blocks = length // BLOCK
    copies = []
    spots = spread(place, far, FAR_STEPS)
    at = 0
    for k, (piece, _, count) in enumerate(spots):
        into = held.at[at : at + count]
        copies.append(pltpu.make_async_copy(piece.at[:, :512], into, done.at[k]))
        copies[-1].start()
        at += count
    moves = []
    for piece, feature, count in spread(place, near + far, NEAR_STEPS + FAR_STEPS):
        base = lax.div(feature, 256) * 256
        first = 2 if piece is far[2] else 0
        for k in range(count // 64):
            to = pl.multiple_of(base + lax.rem(x + first + k, 4) * 64, 64)
            source = piece.at[k * 64 : (k + 1) * 64, 512:768]
            moves.append(
                pltpu.make_async_copy(source, columns_o.at[pl.ds(to, 64)], placed.at[len(moves)])
            )
            moves[-1].start()
    for copy in copies:
        copy.wait()

    def finished(rows, before, columns):
        total, at = before, 0
        for _, feature, count in spots:
            total = total + dot(rows[:, pl.ds(feature, count)], held[at : at + count, columns])
            at += count
        return total

    pre = finished(normed, scores[:, :256], slice(0, 256))
    query[...] = pre[:, :HEAD] * jax.nn.sigmoid(pre[:, :HEAD])
    gate_o[...] = pre[:, HEAD:] * jax.nn.sigmoid(pre[:, HEAD:])

    def gated(rows, before):
        pair = finished(rows, before, slice(256, 512))
        return (pair[:, :HEAD] * jax.nn.sigmoid(pair[:, HEAD:])).astype(BF).astype(F32)

    glu[16 : 16 + length] = gated(normed, scores[:, 256:])
    edge = gated(edges, edge_scores[...])
    glu[:16] = edge[:16]
    glu[16 + length :] = edge[16:]
    framed = glu[...]
    kernel = taps[...].astype(F32)
    total = None
    for r in range(8):
        turned = framed if r == 0 else pltpu.roll(framed, length + 32 - r, 0)
        for j in range(CONV_KW):
            if (1 + j) % 8 == r:
                at = (1 + j) - r
                part = turned[at : at + length] * kernel[j : j + 1]
                total = part if total is None else total + part
    centred = total - jnp.mean(total, axis=-1, keepdims=True)
    variance = jnp.mean(centred * centred, axis=-1, keepdims=True)
    standard = centred * lax.rsqrt(variance + 1e-05) * scale[...].astype(F32)
    conv_o[...] = (standard * jax.nn.sigmoid(standard)).astype(BF)

    t = lax.broadcasted_iota(jnp.int32, (BLOCK, BLOCK), 0)
    s = lax.broadcasted_iota(jnp.int32, (BLOCK, BLOCK), 1)
    for n in range(blocks):
        rows = slice(n * BLOCK, (n + 1) * BLOCK)
        q = query[rows]
        v = values[rows]
        total = jnp.zeros((BLOCK, HEAD), F32)
        for d in range(2):
            lifted = q * grown[d, rows]
            scored = nt(lifted.astype(BF), lowered[d, rows])
            scored = jnp.where(s <= t if d == 0 else s >= t, scored, 0.0)
            total = total + dot(scored.astype(BF), v)
            total = total + nt(lifted.astype(BF), start[d, n])
            lifted_o[d, rows] = (lifted * jnp.exp(passed[d, n : n + 1])).astype(BF)
        local_o[rows] = total
    for move in moves:
        move.wait()


def readout_kernel(place, local, lifted, every, before, rescale, gate, out):
    z = place[0]
    summed = local[...]
    for d in range(2):
        state = jnp.zeros((HEAD, HEAD), F32)
        for k in range(8) if d == 0 else reversed(range(8)):
            new, step = unpack(every[k])
            state = jnp.where(k < z if d == 0 else k > z, jnp.exp(step) * state + new, state)
        incoming = before[d, :HEAD] + jnp.exp(before[d, HEAD : HEAD + 1]) * state
        summed = summed + nt(lifted[d], incoming.astype(BF))
    factor = lax.rsqrt(jnp.mean(summed * summed, axis=-1, keepdims=True) + 1e-06)
    out[...] = (summed * factor * rescale[...].astype(F32) * gate[...]).astype(BF)


def project_out_kernel(place, rec, conv, columns, out):
    core = place[0]
    at = [pl.multiple_of(k * 96 + core * 48, 16) for k in range(4)]
    left = jnp.concatenate([rec[pl.ds(k, 48)] for k in at], axis=0)
    right = jnp.concatenate([conv[pl.ds(k, 48)] for k in at], axis=0)
    rows = jnp.concatenate([left, right], axis=1)
    for c in range(0, 2048, 512):
        part = nt(rows, columns[c : c + 512])
        for k in range(4):
            out[k, :, c : c + 512] = part[k * 48 : (k + 1) * 48].astype(out.dtype)


def meet_kernel(place, mine, got, far_low, far_high, ahead, behind, own):
    y = place[3]

    def block(step):
        k = lax.rem(y + step, 4)
        return mine[k] + got[k].astype(F32)

    far = block(2)
    far_low[...] = far[:, :1024].astype(BF)
    far_high[...] = far[:, 1024:].astype(BF)
    ahead[...] = block(1)
    behind[...] = block(3)
    own[...] = block(0)


def relay_kernel(ahead, behind, low, high, ahead_o, behind_o):
    ahead_o[:, :1024] = (ahead[:, :1024] + low[...].astype(F32)).astype(BF)
    ahead_o[:, 1024:] = ahead[:, 1024:].astype(BF)
    behind_o[:, :1024] = behind[:, :1024].astype(BF)
    behind_o[:, 1024:] = (behind[:, 1024:] + high[...].astype(F32)).astype(BF)


def layer(
    sequence_embeddings,
    entry_rescale_vector,
    probe_matrix,
    onward_retain_matrix,
    reverse_retain_matrix,
    content_matrix,
    emission_switch_matrix,
    pointwise_content_matrix,
    pointwise_switch_matrix,
    retain_lower_slack,
    extra_log_shrink,
    subspace_rescale,
    filter_kernel_coefs,
    channel_cluster_scale,
    scan_readout_matrix,
    filter_readout_matrix,
):
    x, z, y = (lax.axis_index(axis) for axis in "xzy")
    core = lax.axis_index("core")
    length = sequence_embeddings.shape[0]
    gain = entry_rescale_vector[None]
    place = jnp.stack([z, lax.rem(4 - x, 4) * 64, x, y]).astype(jnp.int32)
    edge = pltpu.VMEM((16, sequence_embeddings.shape[1]), BF)
    first, shard, top, bottom = kernel_call(
        collect_kernel,
        2,
        [pltpu.VMEM((8, 64, 384), BF), pltpu.VMEM((64, 768), BF), edge, edge],
        far_off(sequence_embeddings),
        *(
            far_off(weight)
            for weight in (
                onward_retain_matrix,
                reverse_retain_matrix,
                content_matrix,
                probe_matrix,
                emission_switch_matrix,
                pointwise_content_matrix,
                pointwise_switch_matrix,
                scan_readout_matrix.T,
                filter_readout_matrix.T,
            )
        ),
        scratch=(pltpu.SemaphoreType.DMA((2,)),),
        left=(0,),
    )
    first = lax.all_to_all(first, "z", 0, 0, tiled=True)
    first = first.reshape(512, 384)
    ahead, far, behind = shift(shard, "x", -1), shift(shard, "x", 2), shift(shard, "x", 1)
    normed, normed_first = normalized(place, far_off(sequence_embeddings), gain, 2)
    low = line(bottom, ("z", "x"), 1)
    high = line(top, ("z", "x"), -1)
    normed, normed_first, shard, ahead, far, behind, low = lax.optimization_barrier(
        (normed, normed_first, shard, ahead, far, behind, low)
    )
    (edges,) = normalized(place, jnp.concatenate([low, high], axis=0), gain, 1)
    (later,) = kernel_call(
        stack_kernel,
        1,
        [pltpu.HBM((256, 768), BF)],
        keep(shard),
        keep(ahead),
        keep(far),
        keep(behind),
    )
    _, later = ordered(first, later)
    ahead, behind = shift(first, "x", -1), shift(first, "x", 1)
    up1, down1 = shift(later, "z", 1), shift(later, "z", -1)
    far_low, far_high = shift(behind[:256], "x", 1), shift(ahead[256:], "x", -1)
    normed_first = keep(normed_first)
    _, seen = ordered(high, behind)
    (near,) = kernel_call(
        near_scores_kernel,
        2,
        [pltpu.VMEM((length, 384), F32)],
        normed_first,
        keep(first),
        keep(ahead),
        keep(seen),
    )
    _, up1, down1 = ordered(near, up1, down1)
    up2, down2 = shift(up1, "z", 1), shift(down1, "z", -1)
    blocks = length // BLOCK
    values, gap, cum, start, passed, send = kernel_call(
        gates_kernel,
        3,
        [
            pltpu.HBM((length, HEAD), BF),
            pltpu.HBM((2, length, HEAD), F32),
            pltpu.HBM((2, length, HEAD), F32),
            pltpu.HBM((2, blocks, HEAD, HEAD), BF),
            pltpu.HBM((2, 8, HEAD), F32),
            pltpu.VMEM((2, PACK, HEAD), BF),
        ],
        keep(near),
        normed_first,
        keep(far_low),
        keep(far_high),
        retain_lower_slack,
        extra_log_shrink,
    )
    row = [send, shift(send, "x", -1), shift(send, "x", 2), shift(send, "x", 1)]
    _, up2, down2 = ordered(send, up2, down2)
    up3, down3 = shift(up2, "z", 1), shift(down2, "z", -1)
    before, send = kernel_call(
        row_kernel,
        1,
        [pltpu.HBM((2, HEAD + 8, HEAD), F32), pltpu.VMEM((8, PACK, HEAD), BF)],
        place,
        *(keep(piece) for piece in row),
        scratch=(pltpu.VMEM((4, 2, PACK, HEAD), BF),),
    )
    _, up3, down3 = ordered(send, up3, down3)
    low4, high4 = shift(up3[:128], "z", 1), shift(down3[128:], "z", -1)
    every = lax.all_to_all(send, "z", 0, 0, tiled=True)

    near_blocks = [far_off(a) for a in (later, down1, down2, up2, up1)]
    far_blocks = [far_off(down3), low4, high4, far_off(up3)]
    scores, edge_scores, lowered, grown = kernel_call(
        early_kernel,
        3,
        [
            pltpu.HBM((length, 512), F32),
            pltpu.HBM((32, 256), F32),
            pltpu.HBM((2, length, HEAD), BF),
            pltpu.HBM((2, length, HEAD), F32),
        ],
        place,
        far_off(normed),
        keep(edges),
        *near_blocks,
        far_off(gap),
        far_off(cum),
        scratch=(pltpu.VMEM((5, 256, 512), BF), pltpu.SemaphoreType.DMA((5,))),
        left=range(3, 8),
    )
    local, lifted, gate, conv_out, columns = kernel_call(
        later_kernel,
        0.5,
        [
            pltpu.HBM((length, HEAD), F32),
            pltpu.HBM((2, length, HEAD), BF),
            pltpu.HBM((length, HEAD), F32),
            pltpu.VMEM((length, HEAD), BF),
            pltpu.VMEM((2048, 256), BF),
        ],
        place,
        far_off(normed),
        keep(edges),
        far_off(scores),
        far_off(edge_scores),
        *near_blocks,
        *far_blocks,
        *(far_off(a) for a in (values, lowered, grown, start, passed)),
        filter_kernel_coefs,
        channel_cluster_scale[None],
        scratch=(
            pltpu.VMEM((length, HEAD), F32),
            pltpu.VMEM((length + 32, HEAD), F32),
            pltpu.VMEM((768, 512), BF),
            pltpu.SemaphoreType.DMA((4,)),
            pltpu.SemaphoreType.DMA((32,)),
        ),
        left=range(5, 14),
    )
    (rec_out,) = kernel_call(
        readout_kernel,
        1,
        [pltpu.VMEM((length, HEAD), BF)],
        place,
        far_off(local),
        far_off(lifted),
        keep(every),
        far_off(before),
        subspace_rescale[None],
        far_off(gate),
    )
    theirs, mine = (
        kernel_call(
            project_out_kernel,
            1,
            [pltpu.VMEM((4, 48, 2048), kind)],
            side[None].astype(jnp.int32),
            keep(rec_out),
            keep(conv_out),
            keep(columns),
        )[0]
        for side, kind in ((1 - core, BF), (core, F32))
    )
    half, whole, final = (
        pltpu.VMEM((48, 1024), BF),
        pltpu.VMEM((48, 2048), F32),
        pltpu.VMEM((48, 2048), BF),
    )
    far_low, far_high, ahead, behind, own = kernel_call(
        meet_kernel,
        1,
        [half, half, whole, whole, whole],
        place,
        keep(mine),
        keep(shift(theirs, "core", 1)),
    )
    ahead, behind = kernel_call(
        relay_kernel,
        0.5,
        [final, final],
        keep(ahead),
        keep(behind),
        keep(shift(far_low, "y", 1)),
        keep(shift(far_high, "y", -1)),
    )
    ahead, behind = shift(ahead, "y", 1), shift(behind, "y", -1)
    return (own + ahead.astype(F32) + behind.astype(F32)).astype(BF)


def solution(mesh):
    finer = Mesh(mesh.devices.reshape(8, 4, 4, 2), ("z", "x", "y", "core"))
    sp, tp = ("z", "x"), ("y", "core")
    in_specs = (
        P(sp, None),
        P(),
        *(P(sp, tp) for _ in range(7)),
        P(None, tp),
        P(None, sp, tp),
        P(),
        P(None, tp),
        P(tp),
        P(tp, sp),
        P(tp, sp),
    )
    return jax.shard_map(
        layer,
        mesh=finer,
        in_specs=in_specs,
        out_specs=P((*sp, *tp), None),
        check_vma=False,
    )
```

```python
import jax
import jax.numpy as jnp
from jax import lax
from jax.experimental import pallas as pl
from jax.experimental.pallas import tpu as pltpu
from jax.sharding import Mesh
from jax.sharding import PartitionSpec as P


CONV_KW = 31
BLOCK = 64
HEAD = 128
PACK = 144
BF = jnp.bfloat16
F32 = jnp.float32
ROOM = pltpu.CompilerParams(vmem_limit_bytes=24 * 2**20)
SMEM = pl.BlockSpec(memory_space=pltpu.SMEM)
VMEM = pl.BlockSpec(memory_space=pltpu.VMEM)
ANY = pl.BlockSpec(memory_space=pl.ANY)


def ring(count, step):
    return [(i, (i + step) % count) for i in range(count)]


def shift(array, axis, step):
    return lax.ppermute(array, axis, ring(lax.axis_size(axis), step))


def line(array, axes, step):
    count = lax.axis_size(axes)
    pairs = [(i, i + step) for i in range(count) if 0 <= i + step < count]
    return lax.ppermute(array, axes, pairs)


def ordered(first, *arrays):
    return lax.optimization_barrier((first, *arrays))


def keep(array):
    return pltpu.with_memory_space_constraint(array, pltpu.VMEM)


def far_off(array):
    return pltpu.with_memory_space_constraint(array, pltpu.HBM)


def kernel_call(body, micros, outs, *operands, scratch=(), left=()):
    return pl.pallas_call(
        body,
        out_shape=tuple(outs),
        in_specs=[
            SMEM if o.dtype == jnp.int32 else ANY if k in left else VMEM
            for k, o in enumerate(operands)
        ],
        scratch_shapes=list(scratch),
        compiler_params=ROOM,
        cost_estimate=pl.CostEstimate(
            flops=int(micros * 4e6), transcendentals=0, bytes_accessed=0
        ),
    )(*operands)


def nt(a, b):
    return lax.dot_general(a, b, (((1,), (1,)), ((), ())), preferred_element_type=F32)


def tn(a, b):
    return lax.dot_general(a, b, (((0,), (0,)), ((), ())), preferred_element_type=F32)


def dot(a, b):
    return jnp.dot(a, b, preferred_element_type=F32)


def collect_kernel(x, *refs):
    first, later, top, bottom, done = refs[-5:]
    edge = top.shape[0]
    rows = (x.at[:edge], x.at[x.shape[0] - edge :])
    copies = [
        pltpu.make_async_copy(source, into, done.at[k])
        for k, (source, into) in enumerate(zip(rows, (top, bottom)))
    ]
    for copy in copies:
        copy.start()
    for k, ref in enumerate(refs[:3]):
        for z in range(8):
            first[z, :, k * HEAD : (k + 1) * HEAD] = ref[...]
    for k, ref in enumerate(refs[3:-5]):
        later[:, k * HEAD : (k + 1) * HEAD] = ref[...]
    for copy in copies:
        copy.wait()


def stack_kernel(own, ahead, far, behind, later):
    for k, ref in enumerate((own, ahead, far, behind)):
        later[k * 64 : (k + 1) * 64] = ref[...]


def normalize_kernel(place, x, gain, out, *other):
    turn = place[1]
    floats = x[...].astype(F32)
    factor = lax.rsqrt(jnp.mean(floats * floats, axis=-1, keepdims=True) + 1e-06)
    low = lax.broadcasted_iota(jnp.int32, (x.shape[0], HEAD), 1) < 64
    for pair in range(4):
        pieces = []
        for k in (2 * pair, 2 * pair + 1):
            at = slice(k * 256, (k + 1) * 256)
            scaled = x[:, at].astype(F32) * factor * gain[:, at].astype(F32)
            turned = pltpu.roll(scaled, turn, 1)
            out[:, at] = turned.astype(BF)
            pieces.append((turned[:, :HEAD], turned[:, HEAD:]))
        if other:
            for half in range(2):
                one, two = pieces[0][half], pieces[1][half]
                even = jnp.where(low, one, pltpu.roll(two, 64, 1))
                odd = jnp.where(low, pltpu.roll(one, 64, 1), two)
                for piece, value in ((2 * half, even), (2 * half + 1, odd)):
                    at = piece * 512 + pair * HEAD
                    other[0][:, at : at + HEAD] = value.astype(BF)


def normalized(place, x, gain, count):
    outs = [pltpu.VMEM(x.shape, BF), pltpu.VMEM(x.shape, BF)][:count]
    if count == 2:
        outs[0] = pltpu.HBM(x.shape, BF)
    return kernel_call(normalize_kernel, 3, outs, place, x, gain)


def near_scores_kernel(normed, own, ahead, behind, out):
    total = dot(normed[:, :512], own[...])
    total = total + dot(normed[:, 512:1024], ahead[...])
    out[...] = total + dot(normed[:, 1536:], behind[...])


def pack(state, log):
    high = log.astype(BF).astype(F32)
    pad = jnp.zeros((PACK - HEAD - 8, HEAD), F32)
    rows = lax.broadcasted_iota(jnp.int32, (8, HEAD), 0)
    logs = jnp.where(rows == 0, high, jnp.where(rows == 1, log - high, 0.0))
    return jnp.concatenate([state, logs, pad], axis=0).astype(BF)


def unpack(message):
    state = message[:HEAD].astype(F32)
    logs = message[HEAD:PACK].astype(F32)
    return state, logs[0:1] + logs[1:2]


def gates_kernel(near, normed, far_low, far_high, slack, extra, values_o, gap_o, cum_o, start_o, passed_o, send):
    length = near.shape[0]
    blocks = length // BLOCK
    scores = near[...] + dot(normed[:, 1024:1280], far_low[...])
    scores = scores + dot(normed[:, 1280:1536], far_high[...])
    inside = lax.rem(lax.broadcasted_iota(jnp.int32, (length, HEAD), 0), BLOCK)
    v = scores[:, 256:].astype(BF)
    values_o[...] = v
    for d in range(2):
        gap = slack[d : d + 1, :] * jax.nn.sigmoid(-scores[:, d * HEAD : (d + 1) * HEAD])
        cum = jnp.log1p(-gap) + extra[d]
        step = 1
        while step < BLOCK:
            if d == 0:
                moved = jnp.where(inside >= step, pltpu.roll(cum, step, 0), 0.0)
            else:
                moved = jnp.where(inside < BLOCK - step, pltpu.roll(cum, length - step, 0), 0.0)
            cum = cum + moved
            step *= 2
        gap_o[d] = gap
        cum_o[d] = cum
        state = jnp.zeros((HEAD, HEAD), F32)
        passed = jnp.zeros((1, HEAD), F32)
        for n in range(blocks) if d == 0 else reversed(range(blocks)):
            rows = slice(n * BLOCK, (n + 1) * BLOCK)
            last = n * BLOCK + (BLOCK - 1 if d == 0 else 0)
            total = cum[last : last + 1]
            fade = gap[rows] * jnp.exp(total - cum[rows])
            start_o[d, n] = state.astype(BF)
            passed_o[d, n : n + 1] = passed
            state = jnp.exp(total) * state + tn(v[rows], fade.astype(BF))
            passed = passed + total
        send[d] = pack(state, passed)


def row_kernel(place, own, ahead, far, behind, before_o, send, got):
    x, z = place[2], place[0]
    for k, ref in enumerate((own, ahead, far, behind)):
        got[lax.rem(x + k, 4)] = ref[...]
    messages = []
    for d in range(2):
        state = jnp.zeros((HEAD, HEAD), F32)
        log = jnp.zeros((1, HEAD), F32)
        before, passed = state, log
        for k in range(4) if d == 0 else reversed(range(4)):
            before = jnp.where(k == x, state, before)
            passed = jnp.where(k == x, log, passed)
            new, step = unpack(got[k, d])
            state = jnp.exp(step) * state + new
            log = log + step
        before_o[d, :HEAD] = before
        before_o[d, HEAD : HEAD + 8] = jnp.broadcast_to(passed, (8, HEAD))
        messages.append(pack(state, log))
    for k in range(8):
        send[k] = jnp.where(k > z, messages[0], messages[1])


def spread(place, pieces, steps):
    z = place[0]
    found = []
    for piece, (step, inside) in zip(pieces, steps):
        at = pl.multiple_of(lax.rem(z + step, 8) * 256 + inside, 128)
        found.append((piece, at, piece.shape[0]))
    return found


NEAR_STEPS = ((0, 0), (1, 0), (2, 0), (6, 0), (7, 0))
FAR_STEPS = ((3, 0), (4, 0), (4, 128), (5, 0))


def early_kernel(place, normed, edges, *refs):
    pieces = refs[:5]
    gap, cum = refs[5:7]
    scores_o, edge_o, lowered_o, grown_o, held, done = refs[7:]
    copies = []
    for k, piece in enumerate(pieces):
        copies.append(pltpu.make_async_copy(piece.at[:, :512], held.at[k], done.at[k]))
        copies[-1].start()
    for d in range(2):
        grown = jnp.exp(cum[d])
        grown_o[d] = grown
        lowered_o[d] = (gap[d] * jnp.exp(-cum[d])).astype(BF)
    for copy in copies:
        copy.wait()
    total, edge = None, None
    for k, (piece, at, count) in enumerate(spread(place, pieces, NEAR_STEPS)):
        part = dot(normed[:, pl.ds(at, count)], held[k])
        total = part if total is None else total + part
        part = dot(edges[:, pl.ds(at, count)], held[k, :, 256:])
        edge = part if edge is None else edge + part
    scores_o[...] = total
    edge_o[...] = edge


def later_kernel(place, normed, edges, scores, edge_scores, *refs):
    near, far = refs[:5], refs[5:9]
    values_i, start_i, passed, lowered, grown, taps, scale = refs[9:16]
    local_o, lifted_o, gate_o, conv_o, columns_o = refs[16:21]
    query, glu, held, features, values, start, done, placed = refs[21:]
    x = place[2]
    length = normed.shape[0]
    blocks = length // BLOCK
    copies = []
    spots = spread(place, far, FAR_STEPS)
    at = 0
    for piece, feature, count in spots:
        for source, into in (
            (piece.at[:, :512], held.at[at : at + count]),
            (normed.at[:, pl.ds(feature, count)], features.at[:, at : at + count]),
        ):
            copies.append(pltpu.make_async_copy(source, into, done.at[len(copies)]))
            copies[-1].start()
        at += count
    later_copies = [
        pltpu.make_async_copy(values_i, values, done.at[8]),
        pltpu.make_async_copy(start_i, start, done.at[9]),
    ]
    for copy in later_copies:
        copy.start()
    moves = []
    for piece, feature, count in spread(place, near + far, NEAR_STEPS + FAR_STEPS):
        base = lax.div(feature, 256) * 256
        first = 2 if piece is far[2] else 0
        for k in range(count // 64):
            to = pl.multiple_of(base + lax.rem(x + first + k, 4) * 64, 64)
            source = piece.at[k * 64 : (k + 1) * 64, 512:768]
            moves.append(
                pltpu.make_async_copy(source, columns_o.at[pl.ds(to, 64)], placed.at[len(moves)])
            )
            moves[-1].start()
    for copy in copies:
        copy.wait()

    pre = scores[:, :256] + dot(features[...], held[:, :256])
    query[...] = pre[:, :HEAD] * jax.nn.sigmoid(pre[:, :HEAD])
    gate_o[...] = pre[:, HEAD:] * jax.nn.sigmoid(pre[:, HEAD:])

    def gated(pair):
        return (pair[:, :HEAD] * jax.nn.sigmoid(pair[:, HEAD:])).astype(BF).astype(F32)

    glu[16 : 16 + length] = gated(scores[:, 256:] + dot(features[...], held[:, 256:]))
    edge, at = edge_scores[...], 0
    for _, feature, count in spots:
        edge = edge + dot(edges[:, pl.ds(feature, count)], held[at : at + count, 256:])
        at += count
    edge = gated(edge)
    glu[:16] = edge[:16]
    glu[16 + length :] = edge[16:]
    framed = glu[...]
    kernel = taps[...].astype(F32)
    total = None
    for r in range(8):
        turned = framed if r == 0 else pltpu.roll(framed, length + 32 - r, 0)
        for j in range(CONV_KW):
            if (1 + j) % 8 == r:
                at = (1 + j) - r
                part = turned[at : at + length] * kernel[j : j + 1]
                total = part if total is None else total + part
    centred = total - jnp.mean(total, axis=-1, keepdims=True)
    variance = jnp.mean(centred * centred, axis=-1, keepdims=True)
    standard = centred * lax.rsqrt(variance + 1e-05) * scale[...].astype(F32)
    conv_o[...] = (standard * jax.nn.sigmoid(standard)).astype(BF)

    for copy in later_copies:
        copy.wait()
    t = lax.broadcasted_iota(jnp.int32, (BLOCK, BLOCK), 0)
    s = lax.broadcasted_iota(jnp.int32, (BLOCK, BLOCK), 1)
    for n in range(blocks):
        rows = slice(n * BLOCK, (n + 1) * BLOCK)
        q = query[rows]
        v = values[rows]
        total = jnp.zeros((BLOCK, HEAD), F32)
        for d in range(2):
            lifted = q * grown[d, rows]
            scored = nt(lifted.astype(BF), lowered[d, rows])
            scored = jnp.where(s <= t if d == 0 else s >= t, scored, 0.0)
            total = total + dot(scored.astype(BF), v)
            total = total + nt(lifted.astype(BF), start[d, n])
            lifted_o[d, rows] = (lifted * jnp.exp(passed[d, n : n + 1])).astype(BF)
        local_o[rows] = total
    for move in moves:
        move.wait()


def readout_kernel(place, local, lifted, every, before, rescale, gate, out):
    z = place[0]
    summed = local[...]
    for d in range(2):
        state = jnp.zeros((HEAD, HEAD), F32)
        for k in range(8) if d == 0 else reversed(range(8)):
            new, step = unpack(every[k])
            state = jnp.where(k < z if d == 0 else k > z, jnp.exp(step) * state + new, state)
        incoming = before[d, :HEAD] + jnp.exp(before[d, HEAD : HEAD + 1]) * state
        summed = summed + nt(lifted[d], incoming.astype(BF))
    factor = lax.rsqrt(jnp.mean(summed * summed, axis=-1, keepdims=True) + 1e-06)
    out[...] = (summed * factor * rescale[...].astype(F32) * gate[...]).astype(BF)


def project_out_kernel(place, rec, conv, columns, out):
    core = place[0]
    at = [pl.multiple_of(k * 96 + core * 48, 16) for k in range(4)]
    left = jnp.concatenate([rec[pl.ds(k, 48)] for k in at], axis=0)
    right = jnp.concatenate([conv[pl.ds(k, 48)] for k in at], axis=0)
    rows = jnp.concatenate([left, right], axis=1)
    for c in range(0, 2048, 512):
        part = nt(rows, columns[c : c + 512])
        for k in range(4):
            out[k, :, c : c + 512] = part[k * 48 : (k + 1) * 48].astype(out.dtype)


def meet_kernel(place, mine, got, far_low, far_high, ahead, behind, own):
    y = place[3]

    def block(step):
        k = lax.rem(y + step, 4)
        return mine[k] + got[k].astype(F32)

    far = block(2)
    far_low[...] = far[:, :1024].astype(BF)
    far_high[...] = far[:, 1024:].astype(BF)
    ahead[...] = block(1)
    behind[...] = block(3)
    own[...] = block(0)


def relay_kernel(ahead, behind, low, high, ahead_o, behind_o):
    ahead_o[:, :1024] = (ahead[:, :1024] + low[...].astype(F32)).astype(BF)
    ahead_o[:, 1024:] = ahead[:, 1024:].astype(BF)
    behind_o[:, :1024] = behind[:, :1024].astype(BF)
    behind_o[:, 1024:] = (behind[:, 1024:] + high[...].astype(F32)).astype(BF)


def layer(
    sequence_embeddings,
    entry_rescale_vector,
    probe_matrix,
    onward_retain_matrix,
    reverse_retain_matrix,
    content_matrix,
    emission_switch_matrix,
    pointwise_content_matrix,
    pointwise_switch_matrix,
    retain_lower_slack,
    extra_log_shrink,
    subspace_rescale,
    filter_kernel_coefs,
    channel_cluster_scale,
    scan_readout_matrix,
    filter_readout_matrix,
):
    x, z, y = (lax.axis_index(axis) for axis in "xzy")
    core = lax.axis_index("core")
    length = sequence_embeddings.shape[0]
    gain = entry_rescale_vector[None]
    place = jnp.stack([z, lax.rem(4 - x, 4) * 64, x, y]).astype(jnp.int32)
    edge = pltpu.VMEM((16, sequence_embeddings.shape[1]), BF)
    first, shard, top, bottom = kernel_call(
        collect_kernel,
        2,
        [pltpu.VMEM((8, 64, 384), BF), pltpu.VMEM((64, 768), BF), edge, edge],
        far_off(sequence_embeddings),
        *(
            far_off(weight)
            for weight in (
                onward_retain_matrix,
                reverse_retain_matrix,
                content_matrix,
                probe_matrix,
                emission_switch_matrix,
                pointwise_content_matrix,
                pointwise_switch_matrix,
                scan_readout_matrix.T,
                filter_readout_matrix.T,
            )
        ),
        scratch=(pltpu.SemaphoreType.DMA((2,)),),
        left=(0,),
    )
    first = lax.all_to_all(first, "z", 0, 0, tiled=True)
    first = first.reshape(512, 384)
    ahead, far, behind = shift(shard, "x", -1), shift(shard, "x", 2), shift(shard, "x", 1)
    normed, normed_first = normalized(place, far_off(sequence_embeddings), gain, 2)
    low = line(bottom, ("z", "x"), 1)
    high = line(top, ("z", "x"), -1)
    normed, normed_first, shard, ahead, far, behind, low = lax.optimization_barrier(
        (normed, normed_first, shard, ahead, far, behind, low)
    )
    (edges,) = normalized(place, jnp.concatenate([low, high], axis=0), gain, 1)
    (later,) = kernel_call(
        stack_kernel,
        1,
        [pltpu.HBM((256, 768), BF)],
        keep(shard),
        keep(ahead),
        keep(far),
        keep(behind),
    )
    _, later = ordered(first, later)
    ahead, behind = shift(first, "x", -1), shift(first, "x", 1)
    up1, down1 = shift(later, "z", 1), shift(later, "z", -1)
    far_low, far_high = shift(behind[:256], "x", 1), shift(ahead[256:], "x", -1)
    normed_first = keep(normed_first)
    _, seen = ordered(high, behind)
    (near,) = kernel_call(
        near_scores_kernel,
        2,
        [pltpu.VMEM((length, 384), F32)],
        normed_first,
        keep(first),
        keep(ahead),
        keep(seen),
    )
    _, up1, down1 = ordered(near, up1, down1)
    up2, down2 = shift(up1, "z", 1), shift(down1, "z", -1)
    blocks = length // BLOCK
    values, gap, cum, start, passed, send = kernel_call(
        gates_kernel,
        3,
        [
            pltpu.HBM((length, HEAD), BF),
            pltpu.HBM((2, length, HEAD), F32),
            pltpu.HBM((2, length, HEAD), F32),
            pltpu.HBM((2, blocks, HEAD, HEAD), BF),
            pltpu.HBM((2, 8, HEAD), F32),
            pltpu.VMEM((2, PACK, HEAD), BF),
        ],
        keep(near),
        normed_first,
        keep(far_low),
        keep(far_high),
        retain_lower_slack,
        extra_log_shrink,
    )
    row = [send, shift(send, "x", -1), shift(send, "x", 2), shift(send, "x", 1)]
    _, up2, down2 = ordered(send, up2, down2)
    up3, down3 = shift(up2, "z", 1), shift(down2, "z", -1)
    before, send = kernel_call(
        row_kernel,
        1,
        [pltpu.HBM((2, HEAD + 8, HEAD), F32), pltpu.VMEM((8, PACK, HEAD), BF)],
        place,
        *(keep(piece) for piece in row),
        scratch=(pltpu.VMEM((4, 2, PACK, HEAD), BF),),
    )
    _, up3, down3 = ordered(send, up3, down3)
    low4, high4 = shift(up3[:128], "z", 1), shift(down3[128:], "z", -1)
    every = lax.all_to_all(send, "z", 0, 0, tiled=True)

    near_blocks = [far_off(a) for a in (later, down1, down2, up2, up1)]
    far_blocks = [far_off(down3), low4, high4, far_off(up3)]
    scores, edge_scores, lowered, grown = kernel_call(
        early_kernel,
        3,
        [
            pltpu.VMEM((length, 512), F32),
            pltpu.VMEM((32, 256), F32),
            pltpu.VMEM((2, length, HEAD), BF),
            pltpu.VMEM((2, length, HEAD), F32),
        ],
        place,
        far_off(normed),
        keep(edges),
        *near_blocks,
        far_off(gap),
        far_off(cum),
        scratch=(pltpu.VMEM((5, 256, 512), BF), pltpu.SemaphoreType.DMA((5,))),
        left=range(3, 8),
    )
    local, lifted, gate, conv_out, columns = kernel_call(
        later_kernel,
        0.5,
        [
            pltpu.VMEM((length, HEAD), F32),
            pltpu.VMEM((2, length, HEAD), BF),
            pltpu.VMEM((length, HEAD), F32),
            pltpu.VMEM((length, HEAD), BF),
            pltpu.VMEM((2048, 256), BF),
        ],
        place,
        far_off(normed),
        keep(edges),
        keep(scores),
        keep(edge_scores),
        *near_blocks,
        *far_blocks,
        far_off(values),
        far_off(start),
        far_off(passed),
        keep(lowered),
        keep(grown),
        filter_kernel_coefs,
        channel_cluster_scale[None],
        scratch=(
            pltpu.VMEM((length, HEAD), F32),
            pltpu.VMEM((length + 32, HEAD), F32),
            pltpu.VMEM((768, 512), BF),
            pltpu.VMEM((length, 768), BF),
            pltpu.VMEM((length, HEAD), BF),
            pltpu.VMEM((2, blocks, HEAD, HEAD), BF),
            pltpu.SemaphoreType.DMA((10,)),
            pltpu.SemaphoreType.DMA((32,)),
        ),
        left=(1, *range(5, 16)),
    )
    (rec_out,) = kernel_call(
        readout_kernel,
        1,
        [pltpu.VMEM((length, HEAD), BF)],
        place,
        keep(local),
        keep(lifted),
        keep(every),
        far_off(before),
        subspace_rescale[None],
        keep(gate),
    )
    theirs, mine = (
        kernel_call(
            project_out_kernel,
            1,
            [pltpu.VMEM((4, 48, 2048), kind)],
            side[None].astype(jnp.int32),
            keep(rec_out),
            keep(conv_out),
            keep(columns),
        )[0]
        for side, kind in ((1 - core, BF), (core, F32))
    )
    half, whole, final = (
        pltpu.VMEM((48, 1024), BF),
        pltpu.VMEM((48, 2048), F32),
        pltpu.VMEM((48, 2048), BF),
    )
    far_low, far_high, ahead, behind, own = kernel_call(
        meet_kernel,
        1,
        [half, half, whole, whole, whole],
        place,
        keep(mine),
        keep(shift(theirs, "core", 1)),
    )
    ahead, behind = kernel_call(
        relay_kernel,
        0.5,
        [final, final],
        keep(ahead),
        keep(behind),
        keep(shift(far_low, "y", 1)),
        keep(shift(far_high, "y", -1)),
    )
    ahead, behind = shift(ahead, "y", 1), shift(behind, "y", -1)
    return (own + ahead.astype(F32) + behind.astype(F32)).astype(BF)


def solution(mesh):
    finer = Mesh(mesh.devices.reshape(8, 4, 4, 2), ("z", "x", "y", "core"))
    sp, tp = ("z", "x"), ("y", "core")
    in_specs = (
        P(sp, None),
        P(),
        *(P(sp, tp) for _ in range(7)),
        P(None, tp),
        P(None, sp, tp),
        P(),
        P(None, tp),
        P(tp),
        P(tp, sp),
        P(tp, sp),
    )
    return jax.shard_map(
        layer,
        mesh=finer,
        in_specs=in_specs,
        out_specs=P((*sp, *tp), None),
        check_vma=False,
    )
```

```python
import jax
import jax.numpy as jnp
from jax import lax
from jax.experimental import pallas as pl
from jax.experimental.pallas import tpu as pltpu
from jax.sharding import Mesh
from jax.sharding import PartitionSpec as P


CONV_KW = 31
BLOCK = 64
HEAD = 128
PACK = 144
BF = jnp.bfloat16
F32 = jnp.float32
ROOM = pltpu.CompilerParams(vmem_limit_bytes=24 * 2**20)
SMEM = pl.BlockSpec(memory_space=pltpu.SMEM)
VMEM = pl.BlockSpec(memory_space=pltpu.VMEM)
ANY = pl.BlockSpec(memory_space=pl.ANY)


def ring(count, step):
    return [(i, (i + step) % count) for i in range(count)]


def shift(array, axis, step):
    return lax.ppermute(array, axis, ring(lax.axis_size(axis), step))


def line(array, axes, step):
    count = lax.axis_size(axes)
    pairs = [(i, i + step) for i in range(count) if 0 <= i + step < count]
    return lax.ppermute(array, axes, pairs)


def ordered(first, *arrays):
    return lax.optimization_barrier((first, *arrays))


def keep(array):
    return pltpu.with_memory_space_constraint(array, pltpu.VMEM)


def far_off(array):
    return pltpu.with_memory_space_constraint(array, pltpu.HBM)


def kernel_call(body, micros, outs, *operands, scratch=(), left=()):
    return pl.pallas_call(
        body,
        out_shape=tuple(outs),
        in_specs=[
            SMEM if o.dtype == jnp.int32 else ANY if k in left else VMEM
            for k, o in enumerate(operands)
        ],
        scratch_shapes=list(scratch),
        compiler_params=ROOM,
        cost_estimate=pl.CostEstimate(
            flops=int(micros * 4e6), transcendentals=0, bytes_accessed=0
        ),
    )(*operands)


def nt(a, b):
    return lax.dot_general(a, b, (((1,), (1,)), ((), ())), preferred_element_type=F32)


def tn(a, b):
    return lax.dot_general(a, b, (((0,), (0,)), ((), ())), preferred_element_type=F32)


def dot(a, b):
    return jnp.dot(a, b, preferred_element_type=F32)


def collect_first_kernel(a, b, c, first):
    for k, ref in enumerate((a, b, c)):
        for z in range(8):
            first[z, :, k * HEAD : (k + 1) * HEAD] = ref[...]


def collect_kernel(x, *refs):
    later, top, bottom, done = refs[-4:]
    edge = top.shape[0]
    pairs = [(x.at[:edge], top), (x.at[x.shape[0] - edge :], bottom)]
    for k, ref in enumerate(refs[:-4]):
        pairs.append((ref, later.at[:, k * HEAD : (k + 1) * HEAD]))
    copies = [
        pltpu.make_async_copy(source, into, done.at[k]) for k, (source, into) in enumerate(pairs)
    ]
    for copy in copies:
        copy.start()
    for copy in copies:
        copy.wait()


def stack_kernel(own, ahead, far, behind, later):
    for k, ref in enumerate((own, ahead, far, behind)):
        later[k * 64 : (k + 1) * 64] = ref[...]


def normalize_kernel(place, x, gain, out, *other):
    turn = place[1]
    floats = x[...].astype(F32)
    factor = lax.rsqrt(jnp.mean(floats * floats, axis=-1, keepdims=True) + 1e-06)
    low = lax.broadcasted_iota(jnp.int32, (x.shape[0], HEAD), 1) < 64
    for pair in range(4):
        pieces = []
        for k in (2 * pair, 2 * pair + 1):
            at = slice(k * 256, (k + 1) * 256)
            scaled = x[:, at].astype(F32) * factor * gain[:, at].astype(F32)
            turned = pltpu.roll(scaled, turn, 1)
            out[:, at] = turned.astype(BF)
            pieces.append((turned[:, :HEAD], turned[:, HEAD:]))
        if other:
            for half in range(2):
                one, two = pieces[0][half], pieces[1][half]
                even = jnp.where(low, one, pltpu.roll(two, 64, 1))
                odd = jnp.where(low, pltpu.roll(one, 64, 1), two)
                for piece, value in ((2 * half, even), (2 * half + 1, odd)):
                    at = piece * 512 + pair * HEAD
                    other[0][:, at : at + HEAD] = value.astype(BF)


def normalized(place, x, gain, count):
    outs = [pltpu.VMEM(x.shape, BF), pltpu.VMEM(x.shape, BF)][:count]
    if count == 2:
        outs[0] = pltpu.HBM(x.shape, BF)
    return kernel_call(normalize_kernel, 3, outs, place, x, gain)


def near_scores_kernel(normed, own, ahead, behind, out):
    total = dot(normed[:, :512], own[...])
    total = total + dot(normed[:, 512:1024], ahead[...])
    out[...] = total + dot(normed[:, 1536:], behind[...])


def pack(state, log):
    high = log.astype(BF).astype(F32)
    pad = jnp.zeros((PACK - HEAD - 8, HEAD), F32)
    rows = lax.broadcasted_iota(jnp.int32, (8, HEAD), 0)
    logs = jnp.where(rows == 0, high, jnp.where(rows == 1, log - high, 0.0))
    return jnp.concatenate([state, logs, pad], axis=0).astype(BF)


def unpack(message):
    state = message[:HEAD].astype(F32)
    logs = message[HEAD:PACK].astype(F32)
    return state, logs[0:1] + logs[1:2]


def gates_kernel(near, normed, far_low, far_high, slack, extra, values_o, gap_o, cum_o, start_o, passed_o, send):
    length = near.shape[0]
    blocks = length // BLOCK
    scores = near[...] + dot(normed[:, 1024:1280], far_low[...])
    scores = scores + dot(normed[:, 1280:1536], far_high[...])
    inside = lax.rem(lax.broadcasted_iota(jnp.int32, (length, HEAD), 0), BLOCK)
    v = scores[:, 256:].astype(BF)
    values_o[...] = v
    for d in range(2):
        gap = slack[d : d + 1, :] * jax.nn.sigmoid(-scores[:, d * HEAD : (d + 1) * HEAD])
        cum = jnp.log1p(-gap) + extra[d]
        step = 1
        while step < BLOCK:
            if d == 0:
                moved = jnp.where(inside >= step, pltpu.roll(cum, step, 0), 0.0)
            else:
                moved = jnp.where(inside < BLOCK - step, pltpu.roll(cum, length - step, 0), 0.0)
            cum = cum + moved
            step *= 2
        gap_o[d] = gap
        cum_o[d] = cum
        state = jnp.zeros((HEAD, HEAD), F32)
        passed = jnp.zeros((1, HEAD), F32)
        for n in range(blocks) if d == 0 else reversed(range(blocks)):
            rows = slice(n * BLOCK, (n + 1) * BLOCK)
            last = n * BLOCK + (BLOCK - 1 if d == 0 else 0)
            total = cum[last : last + 1]
            fade = gap[rows] * jnp.exp(total - cum[rows])
            start_o[d, n] = state.astype(BF)
            passed_o[d, n : n + 1] = passed
            state = jnp.exp(total) * state + tn(v[rows], fade.astype(BF))
            passed = passed + total
        send[d] = pack(state, passed)


def row_kernel(place, own, ahead, far, behind, before_o, send, got):
    x, z = place[2], place[0]
    for k, ref in enumerate((own, ahead, far, behind)):
        got[lax.rem(x + k, 4)] = ref[...]
    messages = []
    for d in range(2):
        state = jnp.zeros((HEAD, HEAD), F32)
        log = jnp.zeros((1, HEAD), F32)
        before, passed = state, log
        for k in range(4) if d == 0 else reversed(range(4)):
            before = jnp.where(k == x, state, before)
            passed = jnp.where(k == x, log, passed)
            new, step = unpack(got[k, d])
            state = jnp.exp(step) * state + new
            log = log + step
        before_o[d, :HEAD] = before
        before_o[d, HEAD : HEAD + 8] = jnp.broadcast_to(passed, (8, HEAD))
        messages.append(pack(state, log))
    for k in range(8):
        send[k] = jnp.where(k > z, messages[0], messages[1])


def spread(place, pieces, steps):
    z = place[0]
    found = []
    for piece, (step, inside) in zip(pieces, steps):
        at = pl.multiple_of(lax.rem(z + step, 8) * 256 + inside, 128)
        found.append((piece, at, piece.shape[0]))
    return found


NEAR_STEPS = ((0, 0), (1, 0), (2, 0), (6, 0), (7, 0))
FAR_STEPS = ((3, 0), (4, 0), (4, 128), (5, 0))


def early_kernel(place, normed, edges, *refs):
    pieces = refs[:5]
    gap, cum = refs[5:7]
    scores_o, edge_o, lowered_o, grown_o, held, done = refs[7:]
    copies = []
    for k, piece in enumerate(pieces):
        copies.append(pltpu.make_async_copy(piece.at[:, :512], held.at[k], done.at[k]))
        copies[-1].start()
    for d in range(2):
        grown = jnp.exp(cum[d])
        grown_o[d] = grown
        lowered_o[d] = (gap[d] * jnp.exp(-cum[d])).astype(BF)
    for copy in copies:
        copy.wait()
    total, edge = None, None
    for k, (piece, at, count) in enumerate(spread(place, pieces, NEAR_STEPS)):
        part = dot(normed[:, pl.ds(at, count)], held[k])
        total = part if total is None else total + part
        part = dot(edges[:, pl.ds(at, count)], held[k, :, 256:])
        edge = part if edge is None else edge + part
    scores_o[...] = total
    edge_o[...] = edge


def later_kernel(place, normed, edges, scores, edge_scores, *refs):
    near, far = refs[:5], refs[5:9]
    values_i, start_i, passed, lowered, grown, taps, scale = refs[9:16]
    local_o, lifted_o, gate_o, conv_o, columns_o = refs[16:21]
    query, glu, held, features, values, start, done, placed = refs[21:]
    x = place[2]
    length = normed.shape[0]
    blocks = length // BLOCK
    copies = []
    spots = spread(place, far, FAR_STEPS)
    at = 0
    for piece, feature, count in spots:
        for source, into in (
            (piece.at[:, :512], held.at[at : at + count]),
            (normed.at[:, pl.ds(feature, count)], features.at[:, at : at + count]),
        ):
            copies.append(pltpu.make_async_copy(source, into, done.at[len(copies)]))
            copies[-1].start()
        at += count
    later_copies = [
        pltpu.make_async_copy(values_i, values, done.at[8]),
        pltpu.make_async_copy(start_i, start, done.at[9]),
    ]
    for copy in later_copies:
        copy.start()
    moves = []
    for piece, feature, count in spread(place, near + far, NEAR_STEPS + FAR_STEPS):
        base = lax.div(feature, 256) * 256
        first = 2 if piece is far[2] else 0
        for k in range(count // 64):
            to = pl.multiple_of(base + lax.rem(x + first + k, 4) * 64, 64)
            source = piece.at[k * 64 : (k + 1) * 64, 512:768]
            moves.append(
                pltpu.make_async_copy(source, columns_o.at[pl.ds(to, 64)], placed.at[len(moves)])
            )
            moves[-1].start()
    for copy in copies:
        copy.wait()

    pre = scores[:, :256] + dot(features[...], held[:, :256])
    query[...] = pre[:, :HEAD] * jax.nn.sigmoid(pre[:, :HEAD])
    gate_o[...] = pre[:, HEAD:] * jax.nn.sigmoid(pre[:, HEAD:])

    def gated(pair):
        return (pair[:, :HEAD] * jax.nn.sigmoid(pair[:, HEAD:])).astype(BF).astype(F32)

    glu[16 : 16 + length] = gated(scores[:, 256:] + dot(features[...], held[:, 256:]))
    edge, at = edge_scores[...], 0
    for _, feature, count in spots:
        edge = edge + dot(edges[:, pl.ds(feature, count)], held[at : at + count, 256:])
        at += count
    edge = gated(edge)
    glu[:16] = edge[:16]
    glu[16 + length :] = edge[16:]
    framed = glu[...]
    kernel = taps[...].astype(F32)
    total = None
    for r in range(8):
        turned = framed if r == 0 else pltpu.roll(framed, length + 32 - r, 0)
        for j in range(CONV_KW):
            if (1 + j) % 8 == r:
                at = (1 + j) - r
                part = turned[at : at + length] * kernel[j : j + 1]
                total = part if total is None else total + part
    centred = total - jnp.mean(total, axis=-1, keepdims=True)
    variance = jnp.mean(centred * centred, axis=-1, keepdims=True)
    standard = centred * lax.rsqrt(variance + 1e-05) * scale[...].astype(F32)
    conv_o[...] = (standard * jax.nn.sigmoid(standard)).astype(BF)

    for copy in later_copies:
        copy.wait()
    t = lax.broadcasted_iota(jnp.int32, (BLOCK, BLOCK), 0)
    s = lax.broadcasted_iota(jnp.int32, (BLOCK, BLOCK), 1)
    for n in range(blocks):
        rows = slice(n * BLOCK, (n + 1) * BLOCK)
        q = query[rows]
        v = values[rows]
        total = jnp.zeros((BLOCK, HEAD), F32)
        for d in range(2):
            lifted = q * grown[d, rows]
            scored = nt(lifted.astype(BF), lowered[d, rows])
            scored = jnp.where(s <= t if d == 0 else s >= t, scored, 0.0)
            total = total + dot(scored.astype(BF), v)
            total = total + nt(lifted.astype(BF), start[d, n])
            lifted_o[d, rows] = (lifted * jnp.exp(passed[d, n : n + 1])).astype(BF)
        local_o[rows] = total
    for move in moves:
        move.wait()


def readout_kernel(place, local, lifted, every, before, rescale, gate, out):
    z = place[0]
    summed = local[...]
    for d in range(2):
        state = jnp.zeros((HEAD, HEAD), F32)
        for k in range(8) if d == 0 else reversed(range(8)):
            new, step = unpack(every[k])
            state = jnp.where(k < z if d == 0 else k > z, jnp.exp(step) * state + new, state)
        incoming = before[d, :HEAD] + jnp.exp(before[d, HEAD : HEAD + 1]) * state
        summed = summed + nt(lifted[d], incoming.astype(BF))
    factor = lax.rsqrt(jnp.mean(summed * summed, axis=-1, keepdims=True) + 1e-06)
    out[...] = (summed * factor * rescale[...].astype(F32) * gate[...]).astype(BF)


def project_out_kernel(place, rec, conv, columns, out):
    core, first = place[0], place[1]
    count = out.shape[0]
    at = [pl.multiple_of(lax.rem(first + k, 4) * 96 + core * 48, 16) for k in range(count)]
    left = jnp.concatenate([rec[pl.ds(k, 48)] for k in at], axis=0)
    right = jnp.concatenate([conv[pl.ds(k, 48)] for k in at], axis=0)
    rows = jnp.concatenate([left, right], axis=1)
    for c in range(0, 2048, 512):
        part = nt(rows, columns[c : c + 512])
        for k in range(count):
            out[k, :, c : c + 512] = part[k * 48 : (k + 1) * 48].astype(out.dtype)


def meet_far_kernel(mine, got, far_low, far_high):
    far_low[...] = (mine[0, :, :1024] + got[0, :, :1024].astype(F32)).astype(BF)
    far_high[...] = (mine[0, :, 1024:] + got[0, :, 1024:].astype(F32)).astype(BF)


def meet_kernel(mine, got, ahead, behind, own):
    behind[...] = mine[1] + got[0].astype(F32)
    own[...] = mine[2] + got[1].astype(F32)
    ahead[...] = mine[3] + got[2].astype(F32)


def relay_kernel(ahead, behind, low, high, ahead_o, behind_o):
    ahead_o[:, :1024] = (ahead[:, :1024] + low[...].astype(F32)).astype(BF)
    ahead_o[:, 1024:] = ahead[:, 1024:].astype(BF)
    behind_o[:, :1024] = behind[:, :1024].astype(BF)
    behind_o[:, 1024:] = (behind[:, 1024:] + high[...].astype(F32)).astype(BF)


def layer(
    sequence_embeddings,
    entry_rescale_vector,
    probe_matrix,
    onward_retain_matrix,
    reverse_retain_matrix,
    content_matrix,
    emission_switch_matrix,
    pointwise_content_matrix,
    pointwise_switch_matrix,
    retain_lower_slack,
    extra_log_shrink,
    subspace_rescale,
    filter_kernel_coefs,
    channel_cluster_scale,
    scan_readout_matrix,
    filter_readout_matrix,
):
    x, z, y = (lax.axis_index(axis) for axis in "xzy")
    core = lax.axis_index("core")
    length = sequence_embeddings.shape[0]
    gain = entry_rescale_vector[None]
    place = jnp.stack([z, lax.rem(4 - x, 4) * 64, x, y]).astype(jnp.int32)
    edge = pltpu.VMEM((16, sequence_embeddings.shape[1]), BF)
    (first,) = kernel_call(
        collect_first_kernel,
        1,
        [pltpu.HBM((8, 64, 384), BF)],
        far_off(onward_retain_matrix),
        far_off(reverse_retain_matrix),
        far_off(content_matrix),
    )
    shard, top, bottom = kernel_call(
        collect_kernel,
        1,
        [pltpu.VMEM((64, 768), BF), edge, edge],
        far_off(sequence_embeddings),
        *(
            far_off(weight)
            for weight in (
                probe_matrix,
                emission_switch_matrix,
                pointwise_content_matrix,
                pointwise_switch_matrix,
                scan_readout_matrix.T,
                filter_readout_matrix.T,
            )
        ),
        scratch=(pltpu.SemaphoreType.DMA((8,)),),
        left=range(7),
    )
    first = lax.all_to_all(first, "z", 0, 0, tiled=True)
    first = first.reshape(512, 384)
    ahead, far, behind = shift(shard, "x", -1), shift(shard, "x", 2), shift(shard, "x", 1)
    normed, normed_first = normalized(place, far_off(sequence_embeddings), gain, 2)
    low, high = line(bottom, ("z", "x"), 1), line(top, ("z", "x"), -1)
    normed, normed_first, shard, ahead, far, behind = lax.optimization_barrier(
        (normed, normed_first, shard, ahead, far, behind)
    )
    (edges,) = normalized(place, jnp.concatenate([low, high], axis=0), gain, 1)
    (later,) = kernel_call(
        stack_kernel,
        1,
        [pltpu.HBM((256, 768), BF)],
        keep(shard),
        keep(ahead),
        keep(far),
        keep(behind),
    )
    _, later = ordered(first, later)
    ahead, behind = shift(first, "x", -1), shift(first, "x", 1)
    up1, down1 = shift(later, "z", 1), shift(later, "z", -1)
    far_low, far_high = shift(behind[:256], "x", 1), shift(ahead[256:], "x", -1)
    normed_first = keep(normed_first)
    _, _, seen = ordered(low, high, behind)
    (near,) = kernel_call(
        near_scores_kernel,
        2,
        [pltpu.VMEM((length, 384), F32)],
        normed_first,
        keep(first),
        keep(ahead),
        keep(seen),
    )
    _, up1, down1 = ordered(near, up1, down1)
    up2, down2 = shift(up1, "z", 1), shift(down1, "z", -1)
    blocks = length // BLOCK
    values, gap, cum, start, passed, send = kernel_call(
        gates_kernel,
        3,
        [
            pltpu.HBM((length, HEAD), BF),
            pltpu.HBM((2, length, HEAD), F32),
            pltpu.HBM((2, length, HEAD), F32),
            pltpu.HBM((2, blocks, HEAD, HEAD), BF),
            pltpu.HBM((2, 8, HEAD), F32),
            pltpu.VMEM((2, PACK, HEAD), BF),
        ],
        keep(near),
        normed_first,
        keep(far_low),
        keep(far_high),
        retain_lower_slack,
        extra_log_shrink,
    )
    row = [send, shift(send, "x", -1), shift(send, "x", 2), shift(send, "x", 1)]
    _, up2, down2 = ordered(send, up2, down2)
    up3, down3 = shift(up2, "z", 1), shift(down2, "z", -1)
    before, send = kernel_call(
        row_kernel,
        1,
        [pltpu.HBM((2, HEAD + 8, HEAD), F32), pltpu.VMEM((8, PACK, HEAD), BF)],
        place,
        *(keep(piece) for piece in row),
        scratch=(pltpu.VMEM((4, 2, PACK, HEAD), BF),),
    )
    _, up3, down3 = ordered(send, up3, down3)
    low4, high4 = shift(up3[:128], "z", 1), shift(down3[128:], "z", -1)
    every = lax.all_to_all(send, "z", 0, 0, tiled=True)

    near_blocks = [far_off(a) for a in (later, down1, down2, up2, up1)]
    far_blocks = [far_off(down3), low4, high4, far_off(up3)]
    scores, edge_scores, lowered, grown = kernel_call(
        early_kernel,
        3,
        [
            pltpu.VMEM((length, 512), F32),
            pltpu.VMEM((32, 256), F32),
            pltpu.VMEM((2, length, HEAD), BF),
            pltpu.VMEM((2, length, HEAD), F32),
        ],
        place,
        far_off(normed),
        keep(edges),
        *near_blocks,
        far_off(gap),
        far_off(cum),
        scratch=(pltpu.VMEM((5, 256, 512), BF), pltpu.SemaphoreType.DMA((5,))),
        left=range(3, 8),
    )
    local, lifted, gate, conv_out, columns = kernel_call(
        later_kernel,
        0.5,
        [
            pltpu.VMEM((length, HEAD), F32),
            pltpu.VMEM((2, length, HEAD), BF),
            pltpu.VMEM((length, HEAD), F32),
            pltpu.VMEM((length, HEAD), BF),
            pltpu.VMEM((2048, 256), BF),
        ],
        place,
        far_off(normed),
        keep(edges),
        keep(scores),
        keep(edge_scores),
        *near_blocks,
        *far_blocks,
        far_off(values),
        far_off(start),
        far_off(passed),
        keep(lowered),
        keep(grown),
        filter_kernel_coefs,
        channel_cluster_scale[None],
        scratch=(
            pltpu.VMEM((length, HEAD), F32),
            pltpu.VMEM((length + 32, HEAD), F32),
            pltpu.VMEM((768, 512), BF),
            pltpu.VMEM((length, 768), BF),
            pltpu.VMEM((length, HEAD), BF),
            pltpu.VMEM((2, blocks, HEAD, HEAD), BF),
            pltpu.SemaphoreType.DMA((10,)),
            pltpu.SemaphoreType.DMA((32,)),
        ),
        left=(1, *range(5, 16)),
    )
    (rec_out,) = kernel_call(
        readout_kernel,
        1,
        [pltpu.VMEM((length, HEAD), BF)],
        place,
        keep(local),
        keep(lifted),
        keep(every),
        far_off(before),
        subspace_rescale[None],
        keep(gate),
    )

    def projected(side, first, count, kind):
        spot = jnp.stack([side, lax.rem(y + first, 4)]).astype(jnp.int32)
        return kernel_call(
            project_out_kernel,
            count / 4,
            [pltpu.VMEM((count, 48, 2048), kind)],
            spot,
            keep(rec_out),
            keep(conv_out),
            keep(columns),
        )[0]

    half, whole, final = (
        pltpu.VMEM((48, 1024), BF),
        pltpu.VMEM((48, 2048), F32),
        pltpu.VMEM((48, 2048), BF),
    )
    far_got = shift(projected(1 - core, 2, 1, BF), "core", 1)
    rest_got = shift(projected(1 - core, 3, 3, BF), "core", 1)
    mine = keep(projected(core, 2, 4, F32))
    far_low, far_high = kernel_call(meet_far_kernel, 0.3, [half, half], mine, keep(far_got))
    low, high = shift(far_low, "y", 1), shift(far_high, "y", -1)
    ahead, behind, own = kernel_call(meet_kernel, 1, [whole, whole, whole], mine, keep(rest_got))
    ahead, behind = kernel_call(
        relay_kernel, 0.5, [final, final], keep(ahead), keep(behind), keep(low), keep(high)
    )
    ahead, behind = shift(ahead, "y", 1), shift(behind, "y", -1)
    return (own + ahead.astype(F32) + behind.astype(F32)).astype(BF)


def solution(mesh):
    finer = Mesh(mesh.devices.reshape(8, 4, 4, 2), ("z", "x", "y", "core"))
    sp, tp = ("z", "x"), ("y", "core")
    in_specs = (
        P(sp, None),
        P(),
        *(P(sp, tp) for _ in range(7)),
        P(None, tp),
        P(None, sp, tp),
        P(),
        P(None, tp),
        P(tp),
        P(tp, sp),
        P(tp, sp),
    )
    return jax.shard_map(
        layer,
        mesh=finer,
        in_specs=in_specs,
        out_specs=P((*sp, *tp), None),
        check_vma=False,
    )
```

```python
import jax
import jax.numpy as jnp
from jax import lax
from jax.experimental import pallas as pl
from jax.experimental.pallas import tpu as pltpu
from jax.sharding import Mesh
from jax.sharding import PartitionSpec as P


CONV_KW = 31
BLOCK = 64
HEAD = 128
PACK = 144
BF = jnp.bfloat16
F32 = jnp.float32
ROOM = pltpu.CompilerParams(vmem_limit_bytes=24 * 2**20)
SMEM = pl.BlockSpec(memory_space=pltpu.SMEM)
VMEM = pl.BlockSpec(memory_space=pltpu.VMEM)
ANY = pl.BlockSpec(memory_space=pl.ANY)


def ring(count, step):
    return [(i, (i + step) % count) for i in range(count)]


def shift(array, axis, step):
    return lax.ppermute(array, axis, ring(lax.axis_size(axis), step))


def line(array, axes, step):
    count = lax.axis_size(axes)
    pairs = [(i, i + step) for i in range(count) if 0 <= i + step < count]
    return lax.ppermute(array, axes, pairs)


def ordered(first, *arrays):
    return lax.optimization_barrier((first, *arrays))


def keep(array):
    return pltpu.with_memory_space_constraint(array, pltpu.VMEM)


def far_off(array):
    return pltpu.with_memory_space_constraint(array, pltpu.HBM)


def kernel_call(body, micros, outs, *operands, scratch=(), left=()):
    return pl.pallas_call(
        body,
        out_shape=tuple(outs),
        in_specs=[
            SMEM if o.dtype == jnp.int32 else ANY if k in left else VMEM
            for k, o in enumerate(operands)
        ],
        scratch_shapes=list(scratch),
        compiler_params=ROOM,
        cost_estimate=pl.CostEstimate(
            flops=int(micros * 4e6), transcendentals=0, bytes_accessed=0
        ),
    )(*operands)


def nt(a, b):
    return lax.dot_general(a, b, (((1,), (1,)), ((), ())), preferred_element_type=F32)


def tn(a, b):
    return lax.dot_general(a, b, (((0,), (0,)), ((), ())), preferred_element_type=F32)


def dot(a, b):
    return jnp.dot(a, b, preferred_element_type=F32)


def collect_first_kernel(a, b, c, first):
    for k, ref in enumerate((a, b, c)):
        for z in range(8):
            first[z, :, k * HEAD : (k + 1) * HEAD] = ref[...]


def collect_kernel(x, *refs):
    later, top, bottom, done = refs[-4:]
    edge = top.shape[0]
    pairs = [(x.at[:edge], top), (x.at[x.shape[0] - edge :], bottom)]
    for k, ref in enumerate(refs[:-4]):
        pairs.append((ref, later.at[:, k * HEAD : (k + 1) * HEAD]))
    copies = [
        pltpu.make_async_copy(source, into, done.at[k]) for k, (source, into) in enumerate(pairs)
    ]
    for copy in copies:
        copy.start()
    for copy in copies:
        copy.wait()


def stack_kernel(own, ahead, far, behind, later):
    for k, ref in enumerate((own, ahead, far, behind)):
        later[k * 64 : (k + 1) * 64] = ref[...]


def normalize_kernel(place, x, gain, out, *other):
    turn = place[1]
    floats = x[...].astype(F32)
    factor = lax.rsqrt(jnp.mean(floats * floats, axis=-1, keepdims=True) + 1e-06)
    low = lax.broadcasted_iota(jnp.int32, (x.shape[0], HEAD), 1) < 64
    for pair in range(4):
        pieces = []
        for k in (2 * pair, 2 * pair + 1):
            at = slice(k * 256, (k + 1) * 256)
            scaled = x[:, at].astype(F32) * factor * gain[:, at].astype(F32)
            turned = pltpu.roll(scaled, turn, 1)
            out[:, at] = turned.astype(BF)
            pieces.append((turned[:, :HEAD], turned[:, HEAD:]))
        if other:
            for half in range(2):
                one, two = pieces[0][half], pieces[1][half]
                even = jnp.where(low, one, pltpu.roll(two, 64, 1))
                odd = jnp.where(low, pltpu.roll(one, 64, 1), two)
                for piece, value in ((2 * half, even), (2 * half + 1, odd)):
                    at = piece * 512 + pair * HEAD
                    other[0][:, at : at + HEAD] = value.astype(BF)


def normalized(place, x, gain, count):
    outs = [pltpu.VMEM(x.shape, BF), pltpu.VMEM(x.shape, BF)][:count]
    if count == 2:
        outs[0] = pltpu.HBM(x.shape, BF)
    return kernel_call(normalize_kernel, 3, outs, place, x, gain)


def near_scores_kernel(normed, own, ahead, behind, out):
    total = dot(normed[:, :512], own[...])
    total = total + dot(normed[:, 512:1024], ahead[...])
    out[...] = total + dot(normed[:, 1536:], behind[...])


def pack(state, log):
    high = log.astype(BF).astype(F32)
    pad = jnp.zeros((PACK - HEAD - 8, HEAD), F32)
    rows = lax.broadcasted_iota(jnp.int32, (8, HEAD), 0)
    logs = jnp.where(rows == 0, high, jnp.where(rows == 1, log - high, 0.0))
    return jnp.concatenate([state, logs, pad], axis=0).astype(BF)


def unpack(message):
    state = message[:HEAD].astype(F32)
    logs = message[HEAD:PACK].astype(F32)
    return state, logs[0:1] + logs[1:2]


def gates_kernel(near, normed, far_low, far_high, slack, extra, values_o, gap_o, cum_o, start_o, passed_o, send):
    length = near.shape[0]
    blocks = length // BLOCK
    scores = near[...] + dot(normed[:, 1024:1280], far_low[...])
    scores = scores + dot(normed[:, 1280:1536], far_high[...])
    inside = lax.rem(lax.broadcasted_iota(jnp.int32, (length, HEAD), 0), BLOCK)
    v = scores[:, 256:].astype(BF)
    values_o[...] = v
    for d in range(2):
        gap = slack[d : d + 1, :] * jax.nn.sigmoid(-scores[:, d * HEAD : (d + 1) * HEAD])
        cum = jnp.log1p(-gap) + extra[d]
        step = 1
        while step < BLOCK:
            if d == 0:
                moved = jnp.where(inside >= step, pltpu.roll(cum, step, 0), 0.0)
            else:
                moved = jnp.where(inside < BLOCK - step, pltpu.roll(cum, length - step, 0), 0.0)
            cum = cum + moved
            step *= 2
        gap_o[d] = gap
        cum_o[d] = cum
        state = jnp.zeros((HEAD, HEAD), F32)
        passed = jnp.zeros((1, HEAD), F32)
        for n in range(blocks) if d == 0 else reversed(range(blocks)):
            rows = slice(n * BLOCK, (n + 1) * BLOCK)
            last = n * BLOCK + (BLOCK - 1 if d == 0 else 0)
            total = cum[last : last + 1]
            fade = gap[rows] * jnp.exp(total - cum[rows])
            start_o[d, n] = state.astype(BF)
            passed_o[d, n : n + 1] = passed
            state = jnp.exp(total) * state + tn(v[rows], fade.astype(BF))
            passed = passed + total
        send[d] = pack(state, passed)


def row_kernel(place, own, ahead, far, behind, before_o, send, got):
    x, z = place[2], place[0]
    for k, ref in enumerate((own, ahead, far, behind)):
        got[lax.rem(x + k, 4)] = ref[...]
    messages = []
    for d in range(2):
        state = jnp.zeros((HEAD, HEAD), F32)
        log = jnp.zeros((1, HEAD), F32)
        before, passed = state, log
        for k in range(4) if d == 0 else reversed(range(4)):
            before = jnp.where(k == x, state, before)
            passed = jnp.where(k == x, log, passed)
            new, step = unpack(got[k, d])
            state = jnp.exp(step) * state + new
            log = log + step
        before_o[d, :HEAD] = before
        before_o[d, HEAD : HEAD + 8] = jnp.broadcast_to(passed, (8, HEAD))
        messages.append(pack(state, log))
    for k in range(8):
        send[k] = jnp.where(k > z, messages[0], messages[1])


def spread(place, pieces, steps):
    z = place[0]
    found = []
    for piece, (step, inside) in zip(pieces, steps):
        at = pl.multiple_of(lax.rem(z + step, 8) * 256 + inside, 128)
        found.append((piece, at, piece.shape[0]))
    return found


NEAR_STEPS = ((0, 0), (1, 0), (2, 0), (6, 0), (7, 0))
FAR_STEPS = ((3, 0), (4, 0), (4, 128), (5, 0))


def early_kernel(place, normed, edges, *refs):
    pieces = refs[:5]
    gap, cum = refs[5:7]
    scores_o, edge_o, lowered_o, grown_o, held, done = refs[7:]
    copies = []
    for k, piece in enumerate(pieces):
        copies.append(pltpu.make_async_copy(piece.at[:, :512], held.at[k], done.at[k]))
        copies[-1].start()
    for d in range(2):
        grown = jnp.exp(cum[d])
        grown_o[d] = grown
        lowered_o[d] = (gap[d] * jnp.exp(-cum[d])).astype(BF)
    for copy in copies:
        copy.wait()
    total, edge = None, None
    for k, (piece, at, count) in enumerate(spread(place, pieces, NEAR_STEPS)):
        part = dot(normed[:, pl.ds(at, count)], held[k])
        total = part if total is None else total + part
        part = dot(edges[:, pl.ds(at, count)], held[k, :, 256:])
        edge = part if edge is None else edge + part
    scores_o[...] = total
    edge_o[...] = edge


def later_kernel(place, normed, edges, scores, edge_scores, *refs):
    near, far = refs[:5], refs[5:9]
    values_i, start_i, passed, lowered, grown, taps, scale = refs[9:16]
    local_o, lifted_o, gate_o, conv_o, columns_o = refs[16:21]
    query, glu, held, features, values, start, done, placed = refs[21:]
    x = place[2]
    length = normed.shape[0]
    blocks = length // BLOCK
    copies = []
    spots = spread(place, far, FAR_STEPS)
    at = 0
    for piece, feature, count in spots:
        for source, into in (
            (piece.at[:, :512], held.at[at : at + count]),
            (normed.at[:, pl.ds(feature, count)], features.at[:, at : at + count]),
        ):
            copies.append(pltpu.make_async_copy(source, into, done.at[len(copies)]))
            copies[-1].start()
        at += count
    later_copies = [
        pltpu.make_async_copy(values_i, values, done.at[8]),
        pltpu.make_async_copy(start_i, start, done.at[9]),
    ]
    for copy in later_copies:
        copy.start()
    moves = []
    for piece, feature, count in spread(place, near + far, NEAR_STEPS + FAR_STEPS):
        base = lax.div(feature, 256) * 256
        first = 2 if piece is far[2] else 0
        for k in range(count // 64):
            to = pl.multiple_of(base + lax.rem(x + first + k, 4) * 64, 64)
            source = piece.at[k * 64 : (k + 1) * 64, 512:768]
            moves.append(
                pltpu.make_async_copy(source, columns_o.at[pl.ds(to, 64)], placed.at[len(moves)])
            )
            moves[-1].start()
    for copy in copies:
        copy.wait()

    pre = scores[:, :256] + dot(features[...], held[:, :256])
    query[...] = pre[:, :HEAD] * jax.nn.sigmoid(pre[:, :HEAD])
    gate_o[...] = pre[:, HEAD:] * jax.nn.sigmoid(pre[:, HEAD:])

    def gated(pair):
        return (pair[:, :HEAD] * jax.nn.sigmoid(pair[:, HEAD:])).astype(BF).astype(F32)

    glu[16 : 16 + length] = gated(scores[:, 256:] + dot(features[...], held[:, 256:]))
    edge, at = edge_scores[...], 0
    for _, feature, count in spots:
        edge = edge + dot(edges[:, pl.ds(feature, count)], held[at : at + count, 256:])
        at += count
    edge = gated(edge)
    glu[:16] = edge[:16]
    glu[16 + length :] = edge[16:]
    framed = glu[...]
    kernel = taps[...].astype(F32)
    total = None
    for r in range(8):
        turned = framed if r == 0 else pltpu.roll(framed, length + 32 - r, 0)
        for j in range(CONV_KW):
            if (1 + j) % 8 == r:
                at = (1 + j) - r
                part = turned[at : at + length] * kernel[j : j + 1]
                total = part if total is None else total + part
    centred = total - jnp.mean(total, axis=-1, keepdims=True)
    variance = jnp.mean(centred * centred, axis=-1, keepdims=True)
    standard = centred * lax.rsqrt(variance + 1e-05) * scale[...].astype(F32)
    conv_o[...] = (standard * jax.nn.sigmoid(standard)).astype(BF)

    for copy in later_copies:
        copy.wait()
    t = lax.broadcasted_iota(jnp.int32, (BLOCK, BLOCK), 0)
    s = lax.broadcasted_iota(jnp.int32, (BLOCK, BLOCK), 1)
    for n in range(blocks):
        rows = slice(n * BLOCK, (n + 1) * BLOCK)
        q = query[rows]
        v = values[rows]
        total = jnp.zeros((BLOCK, HEAD), F32)
        for d in range(2):
            lifted = q * grown[d, rows]
            scored = nt(lifted.astype(BF), lowered[d, rows])
            scored = jnp.where(s <= t if d == 0 else s >= t, scored, 0.0)
            total = total + dot(scored.astype(BF), v)
            total = total + nt(lifted.astype(BF), start[d, n])
            lifted_o[d, rows] = (lifted * jnp.exp(passed[d, n : n + 1])).astype(BF)
        local_o[rows] = total
    for move in moves:
        move.wait()


def readout_kernel(place, local, lifted, every, before, rescale, gate, out):
    z = place[0]
    summed = local[...]
    for d in range(2):
        state = jnp.zeros((HEAD, HEAD), F32)
        for k in range(8) if d == 0 else reversed(range(8)):
            new, step = unpack(every[k])
            state = jnp.where(k < z if d == 0 else k > z, jnp.exp(step) * state + new, state)
        incoming = before[d, :HEAD] + jnp.exp(before[d, HEAD : HEAD + 1]) * state
        summed = summed + nt(lifted[d], incoming.astype(BF))
    factor = lax.rsqrt(jnp.mean(summed * summed, axis=-1, keepdims=True) + 1e-06)
    out[...] = (summed * factor * rescale[...].astype(F32) * gate[...]).astype(BF)


def project_out_kernel(place, rec, conv, columns, out):
    core = place[0]
    at = [pl.multiple_of(k * 96 + core * 48, 16) for k in range(4)]
    left = jnp.concatenate([rec[pl.ds(k, 48)] for k in at], axis=0)
    right = jnp.concatenate([conv[pl.ds(k, 48)] for k in at], axis=0)
    rows = jnp.concatenate([left, right], axis=1)
    for c in range(0, 2048, 512):
        part = nt(rows, columns[c : c + 512])
        for k in range(4):
            out[k, :, c : c + 512] = part[k * 48 : (k + 1) * 48].astype(out.dtype)


def meet_kernel(place, mine, got, far_low, far_high, ahead, behind, own):
    y = place[3]

    def block(step):
        k = lax.rem(y + step, 4)
        return mine[k] + got[k].astype(F32)

    far = block(2)
    far_low[...] = far[:, :1024].astype(BF)
    far_high[...] = far[:, 1024:].astype(BF)
    ahead[...] = block(1)
    behind[...] = block(3)
    own[...] = block(0)


def relay_kernel(ahead, behind, low, high, ahead_o, behind_o):
    ahead_o[:, :1024] = (ahead[:, :1024] + low[...].astype(F32)).astype(BF)
    ahead_o[:, 1024:] = ahead[:, 1024:].astype(BF)
    behind_o[:, :1024] = behind[:, :1024].astype(BF)
    behind_o[:, 1024:] = (behind[:, 1024:] + high[...].astype(F32)).astype(BF)


def layer(
    sequence_embeddings,
    entry_rescale_vector,
    probe_matrix,
    onward_retain_matrix,
    reverse_retain_matrix,
    content_matrix,
    emission_switch_matrix,
    pointwise_content_matrix,
    pointwise_switch_matrix,
    retain_lower_slack,
    extra_log_shrink,
    subspace_rescale,
    filter_kernel_coefs,
    channel_cluster_scale,
    scan_readout_matrix,
    filter_readout_matrix,
):
    x, z, y = (lax.axis_index(axis) for axis in "xzy")
    core = lax.axis_index("core")
    length = sequence_embeddings.shape[0]
    gain = entry_rescale_vector[None]
    place = jnp.stack([z, lax.rem(4 - x, 4) * 64, x, y]).astype(jnp.int32)
    edge = pltpu.VMEM((16, sequence_embeddings.shape[1]), BF)
    (first,) = kernel_call(
        collect_first_kernel,
        1,
        [pltpu.HBM((8, 64, 384), BF)],
        far_off(onward_retain_matrix),
        far_off(reverse_retain_matrix),
        far_off(content_matrix),
    )
    shard, top, bottom = kernel_call(
        collect_kernel,
        1,
        [pltpu.VMEM((64, 768), BF), edge, edge],
        far_off(sequence_embeddings),
        *(
            far_off(weight)
            for weight in (
                probe_matrix,
                emission_switch_matrix,
                pointwise_content_matrix,
                pointwise_switch_matrix,
                scan_readout_matrix.T,
                filter_readout_matrix.T,
            )
        ),
        scratch=(pltpu.SemaphoreType.DMA((8,)),),
        left=range(7),
    )
    first = lax.all_to_all(first, "z", 0, 0, tiled=True)
    first = first.reshape(512, 384)
    ahead, far, behind = shift(shard, "x", -1), shift(shard, "x", 2), shift(shard, "x", 1)
    normed, normed_first = normalized(place, far_off(sequence_embeddings), gain, 2)
    low, high = line(bottom, ("z", "x"), 1), line(top, ("z", "x"), -1)
    normed, normed_first, shard, ahead, far, behind = lax.optimization_barrier(
        (normed, normed_first, shard, ahead, far, behind)
    )
    (edges,) = normalized(place, jnp.concatenate([low, high], axis=0), gain, 1)
    (later,) = kernel_call(
        stack_kernel,
        1,
        [pltpu.HBM((256, 768), BF)],
        keep(shard),
        keep(ahead),
        keep(far),
        keep(behind),
    )
    _, later = ordered(first, later)
    ahead, behind = shift(first, "x", -1), shift(first, "x", 1)
    up1, down1 = shift(later, "z", 1), shift(later, "z", -1)
    far_low, far_high = shift(behind[:256], "x", 1), shift(ahead[256:], "x", -1)
    normed_first = keep(normed_first)
    _, _, seen = ordered(low, high, behind)
    (near,) = kernel_call(
        near_scores_kernel,
        2,
        [pltpu.VMEM((length, 384), F32)],
        normed_first,
        keep(first),
        keep(ahead),
        keep(seen),
    )
    _, up1, down1 = ordered(near, up1, down1)
    up2, down2 = shift(up1, "z", 1), shift(down1, "z", -1)
    blocks = length // BLOCK
    values, gap, cum, start, passed, send = kernel_call(
        gates_kernel,
        3,
        [
            pltpu.HBM((length, HEAD), BF),
            pltpu.HBM((2, length, HEAD), F32),
            pltpu.HBM((2, length, HEAD), F32),
            pltpu.HBM((2, blocks, HEAD, HEAD), BF),
            pltpu.HBM((2, 8, HEAD), F32),
            pltpu.VMEM((2, PACK, HEAD), BF),
        ],
        keep(near),
        normed_first,
        keep(far_low),
        keep(far_high),
        retain_lower_slack,
        extra_log_shrink,
    )
    row = [send, shift(send, "x", -1), shift(send, "x", 2), shift(send, "x", 1)]
    _, up2, down2 = ordered(send, up2, down2)
    up3, down3 = shift(up2, "z", 1), shift(down2, "z", -1)
    before, send = kernel_call(
        row_kernel,
        1,
        [pltpu.HBM((2, HEAD + 8, HEAD), F32), pltpu.VMEM((8, PACK, HEAD), BF)],
        place,
        *(keep(piece) for piece in row),
        scratch=(pltpu.VMEM((4, 2, PACK, HEAD), BF),),
    )
    _, up3, down3 = ordered(send, up3, down3)
    low4, high4 = shift(up3[:128], "z", 1), shift(down3[128:], "z", -1)
    every = lax.all_to_all(send, "z", 0, 0, tiled=True)

    near_blocks = [far_off(a) for a in (later, down1, down2, up2, up1)]
    far_blocks = [far_off(down3), low4, high4, far_off(up3)]
    scores, edge_scores, lowered, grown = kernel_call(
        early_kernel,
        3,
        [
            pltpu.VMEM((length, 512), F32),
            pltpu.VMEM((32, 256), F32),
            pltpu.VMEM((2, length, HEAD), BF),
            pltpu.VMEM((2, length, HEAD), F32),
        ],
        place,
        far_off(normed),
        keep(edges),
        *near_blocks,
        far_off(gap),
        far_off(cum),
        scratch=(pltpu.VMEM((5, 256, 512), BF), pltpu.SemaphoreType.DMA((5,))),
        left=range(3, 8),
    )
    local, lifted, gate, conv_out, columns = kernel_call(
        later_kernel,
        0.5,
        [
            pltpu.VMEM((length, HEAD), F32),
            pltpu.VMEM((2, length, HEAD), BF),
            pltpu.VMEM((length, HEAD), F32),
            pltpu.VMEM((length, HEAD), BF),
            pltpu.VMEM((2048, 256), BF),
        ],
        place,
        far_off(normed),
        keep(edges),
        keep(scores),
        keep(edge_scores),
        *near_blocks,
        *far_blocks,
        far_off(values),
        far_off(start),
        far_off(passed),
        keep(lowered),
        keep(grown),
        filter_kernel_coefs,
        channel_cluster_scale[None],
        scratch=(
            pltpu.VMEM((length, HEAD), F32),
            pltpu.VMEM((length + 32, HEAD), F32),
            pltpu.VMEM((768, 512), BF),
            pltpu.VMEM((length, 768), BF),
            pltpu.VMEM((length, HEAD), BF),
            pltpu.VMEM((2, blocks, HEAD, HEAD), BF),
            pltpu.SemaphoreType.DMA((10,)),
            pltpu.SemaphoreType.DMA((32,)),
        ),
        left=(1, *range(5, 16)),
    )
    (rec_out,) = kernel_call(
        readout_kernel,
        1,
        [pltpu.VMEM((length, HEAD), BF)],
        place,
        keep(local),
        keep(lifted),
        keep(every),
        far_off(before),
        subspace_rescale[None],
        keep(gate),
    )
    theirs, mine = (
        kernel_call(
            project_out_kernel,
            1,
            [pltpu.VMEM((4, 48, 2048), kind)],
            side[None].astype(jnp.int32),
            keep(rec_out),
            keep(conv_out),
            keep(columns),
        )[0]
        for side, kind in ((1 - core, BF), (core, F32))
    )
    half, whole, final = (
        pltpu.VMEM((48, 1024), BF),
        pltpu.VMEM((48, 2048), F32),
        pltpu.VMEM((48, 2048), BF),
    )
    far_low, far_high, ahead, behind, own = kernel_call(
        meet_kernel,
        1,
        [half, half, whole, whole, whole],
        place,
        keep(mine),
        keep(shift(theirs, "core", 1)),
    )
    ahead, behind = kernel_call(
        relay_kernel,
        0.5,
        [final, final],
        keep(ahead),
        keep(behind),
        keep(shift(far_low, "y", 1)),
        keep(shift(far_high, "y", -1)),
    )
    ahead, behind = shift(ahead, "y", 1), shift(behind, "y", -1)
    return (own + ahead.astype(F32) + behind.astype(F32)).astype(BF)


def solution(mesh):
    finer = Mesh(mesh.devices.reshape(8, 4, 4, 2), ("z", "x", "y", "core"))
    sp, tp = ("z", "x"), ("y", "core")
    in_specs = (
        P(sp, None),
        P(),
        *(P(sp, tp) for _ in range(7)),
        P(None, tp),
        P(None, sp, tp),
        P(),
        P(None, tp),
        P(tp),
        P(tp, sp),
        P(tp, sp),
    )
    return jax.shard_map(
        layer,
        mesh=finer,
        in_specs=in_specs,
        out_specs=P((*sp, *tp), None),
        check_vma=False,
    )
```
